32 devices in a mesh: sp: 8 (over z, y), tp: 4 (over x, core).
Axes of the slice: x: 2, y: 2, z: 4, core: 2. Of those that a mesh axis runs over, the one named last changes fastest.
Arguments:
- queries: bfloat16 [6144, 1024], P('sp', 'tp'), may hold values from -6 to 6
- keys: bfloat16 [6144, 1024], P('sp', 'tp'), may hold values from -6 to 6
- values: bfloat16 [6144, 2048], P('sp', 'tp'), may hold values from -6 to 6
- out_gate: bfloat16 [6144, 2048], P('sp', 'tp'), may hold values from -6 to 6
- input_gates: float32 [2, 4, 6144], P(None, 'tp', 'sp'), may hold values from -4 to 300
- forget_gates: float32 [2, 4, 6144], P(None, 'tp', 'sp'), may hold values from -1 to 16
- doc_ids: int32 [6144], P('sp'), may hold values from 0 to 3, never falling along the last dimension, each value on 1 to 3072 neighbouring positions
- head_gain: float32 [2048], P('tp'), may hold values from 0.1 to 1.9
- w_out: bfloat16 [2048, 2048], P('tp'), may hold values from -0.25 to 0.25
- resid: bfloat16 [6144, 2048], P(('sp', 'tp')), may hold values from -30 to 30
- norm_gain: float32 [2048], replicated, may hold values from 0.1 to 1.9
- w_up: bfloat16 [2048, 8192], P('sp', 'tp'), may hold values from -0.125 to 0.125
- w_down: bfloat16 [8192, 2048], P('tp', 'sp'), may hold values from -0.0625 to 0.0625
Outputs:
- layer_out: bfloat16 [6144, 2048], P(('sp', 'tp'))
The draws below stay inside these ranges and needn't reach their ends.
Inputs may be any that keep to these rules, and one draw needn't show every extreme that they name: `doc_ids`: document numbers never fall along the positions.
All inputs are finite; a program needn't handle non-finite values.
Results may differ from the reference program's by a relative error of at most 0.013.
Values may be sent and summed in bfloat16 or wider, within the bound.
No kernel may reach another device: no remote copies, remote signals or barrier semaphores. Data moves between devices by JAX's collectives and lax.ppermute only.
A program may use at most 128 MiB of HBM per device.

```python
import math
import jax
import jax.numpy as jnp
import numpy as np
from jax import lax

D = 2048
HEADS = 4
DQK = 256
DV = 512
FF = 8192
TOK_DEV = 768
TOKENS = 6144
N_SP = 8


def draw_resid(key, part):
    keys = jax.random.split(key, 2)
    base = jax.random.normal(keys[0], (TOKENS, D), jnp.float32)
    rows = jnp.exp(jax.random.uniform(keys[1], (TOKENS, 1), jnp.float32, -1.2, 1.2))
    cols = jnp.exp(jnp.linspace(-0.9, 0.9, D, dtype=jnp.float32))[None, :]
    return jnp.clip(base * rows * cols, -30.0, 30.0).astype(jnp.bfloat16)


def draw_input_gates(key, part):
    keys = jax.random.split(key, 1)
    gates = jnp.clip(jax.random.normal(keys[0], (2, HEADS, TOKENS), jnp.float32), -4.0, 4.0)
    return gates


def draw_forget_gates(key, part):
    keys = jax.random.split(key, 6)
    share = 0.5
    slow = jax.random.uniform(keys[0], (2, HEADS, 1), jnp.float32) < share
    fast_rate = jnp.exp(jax.random.uniform(keys[1], (2, HEADS, 1), jnp.float32, jnp.log(1.0 / 100.0), jnp.log(1.0 / 30.0)))
    rate = jnp.where(slow, 0.3 / TOKENS, fast_rate)
    factor = jnp.exp(jax.random.uniform(keys[2], (2, HEADS, TOKENS // TOK_DEV), jnp.float32, -0.7, 0.7))
    factor = jnp.repeat(factor, TOK_DEV, axis=2)
    noise = jnp.clip(jax.random.normal(keys[3], (2, HEADS, TOKENS), jnp.float32), -3.0, 3.0)
    pre = -jnp.log(rate * factor) + noise
    spots = jax.random.randint(keys[4], (2, HEADS, 3), 0, TOKENS)
    hit = jnp.any(jnp.arange(TOKENS)[None, None, None, :] == spots[..., None], axis=2)
    drop = jax.random.uniform(keys[5], (2, HEADS, TOKENS), jnp.float32, 0.0, 1.4)
    return jnp.where(hit, drop, pre)


def shard_levels(stream_key, extent, cuts, least, high):
    def one(axis_at, shards_of):
        steps = jax.random.uniform(jax.random.fold_in(jax.random.fold_in(stream_key, 6), axis_at), (shards_of,), jnp.float32, least / len(cuts), high / len(cuts))
        return jnp.repeat(jnp.exp(steps), extent[axis_at] // shards_of).reshape((-1,) + (1,) * (len(extent) - axis_at - 1))

    gain = one(*cuts[0])
    for cut in cuts[1:]:
        gain = gain * one(*cut)
    return gain


def profile(amount, total, limit, skew):
    loads = [(1 << 20) // math.isqrt(rank ** skew) + 1 for rank in range(2, amount + 1)]
    rest, holding = total - limit - (amount - 1), [1] * (amount - 1)
    while rest > 0:
        candidates = [i for i in range(amount - 1) if holding[i] < limit]
        pool, budget = sum([loads[i] for i in candidates]), rest
        for i in candidates:
            addition = min(limit - holding[i], max(1, budget * loads[i] // pool), rest)
            holding[i] = holding[i] + addition
            rest = rest - addition
    return np.array([limit] + holding)


def uneven_parts(own_key, count, total, bound, lean):
    if count == 2:
        one = jax.random.randint(own_key, (), max(1, total - bound), min(bound, total - 1) + 1)
        return jnp.stack([one, total - one])
    tallies = jnp.asarray(profile(count, total, bound, lean), jnp.int32)
    pairs = (count - 1) // 2
    source_of, sink = tallies[1:1 + 2 * pairs:2], tallies[2:2 + 2 * pairs:2]
    room = jnp.minimum(source_of - 1, bound - sink)
    moved = jax.random.randint(jax.random.fold_in(own_key, 1), (pairs,), 0, 1 << 20) % (room + 1)
    tallies = tallies.at[1:1 + 2 * pairs:2].set(source_of - moved).at[2:2 + 2 * pairs:2].set(sink + moved)
    return tallies[jax.random.permutation(jax.random.fold_in(own_key, 2), count)]


def gaussian(key, shape, deviation, most, cuts=(), kind=jnp.bfloat16):
    entries = deviation * jax.random.normal(key, shape, jnp.float32)
    if cuts:
        entries = entries * shard_levels(key, shape, cuts, -0.22, 0.18)
    return jnp.clip(entries, -most, most).astype(kind)


def setup_inputs(seed: int = 0) -> dict:
    arg_keys = jax.random.split(jax.random.key(seed), 14)
    queries = gaussian(arg_keys[0], (TOKENS, HEADS * DQK), 1.0, 6.0, ((0, 8), (1, 4)))
    keys = gaussian(arg_keys[1], (TOKENS, HEADS * DQK), 1.0, 6.0, ((0, 8), (1, 4)))
    values = gaussian(arg_keys[2], (TOKENS, HEADS * DV), 1.0, 6.0, ((0, 8), (1, 4)))
    out_gate = gaussian(arg_keys[3], (TOKENS, HEADS * DV), 1.0, 6.0, ((0, 8), (1, 4)))
    input_gates = draw_input_gates(jax.random.fold_in(arg_keys[13], 71), 0)
    forget_gates = draw_forget_gates(jax.random.fold_in(arg_keys[13], 71), 0)
    doc_ids = jnp.searchsorted(jnp.cumsum(uneven_parts(arg_keys[6], N_SP // 2, TOKENS, 4 * TOK_DEV, 0)), jnp.arange(TOKENS), side="right").astype(jnp.int32)
    head_gain = jnp.clip(1.0 + 0.18 * jax.random.normal(arg_keys[7], (HEADS * DV,), jnp.float32), 0.1, 1.9)
    w_out = gaussian(arg_keys[8], (HEADS * DV, D), (HEADS * DV // 4) ** -0.5, 0.25, ((0, 4),))
    resid = draw_resid(jax.random.fold_in(arg_keys[13], 71), 0)
    norm_gain = jnp.clip(1.0 + 0.18 * jax.random.normal(arg_keys[10], (D,), jnp.float32), 0.1, 1.9)
    w_up = gaussian(arg_keys[11], (D, FF), D ** -0.5, 0.125, ((0, 8), (1, 4)))
    w_down = gaussian(arg_keys[12], (FF, D), FF ** -0.5, 0.0625, ((0, 4), (1, 8)))
    return dict(queries=queries, keys=keys, values=values, out_gate=out_gate, input_gates=input_gates, forget_gates=forget_gates, doc_ids=doc_ids, head_gain=head_gain, w_out=w_out, resid=resid, norm_gain=norm_gain, w_up=w_up, w_down=w_down)


eps = 1e-06
far_low = -1e+30

def summarize(keys_blk, values_blk, in_gate, forget_pre, doc_pos):
    logf = jax.nn.log_sigmoid(forget_pre)
    cum = jnp.cumsum(logf)
    length = keys_blk.shape[0]
    last_doc = doc_pos[length - 1]
    tail = doc_pos == last_doc
    total = cum[length - 1]
    exponent = jnp.where(tail, total - cum + in_gate, far_low)
    peak = jnp.max(exponent)
    scaled = jnp.exp(exponent - peak)
    weighted = (keys_blk.astype(jnp.float32) * scaled[:, None]).astype(jnp.bfloat16)
    memory = jnp.einsum('sd,sv->dv', weighted.astype(jnp.float32), values_blk.astype(jnp.float32))
    norm_keys = lax.optimization_barrier(jnp.sum(weighted.astype(jnp.float32), axis=0))
    return (memory, norm_keys, peak, total, doc_pos[0], last_doc, jnp.zeros((), jnp.float32))

def emit(queries_blk, keys_blk, values_blk, in_gate, forget_pre, doc_pos, state):
    memory, norm_keys, top_in, total_in, first_in, last_in, empty_in = state
    scale = queries_blk.shape[1] ** (-0.5)
    logf = jax.nn.log_sigmoid(forget_pre)
    cum = jnp.cumsum(logf)
    length = queries_blk.shape[0]
    place = jnp.arange(length)
    keep = (place[:, None] >= place[None, :]) & (doc_pos[:, None] == doc_pos[None, :])
    exponent = jnp.where(keep, cum[:, None] - cum[None, :] + in_gate[None, :], far_low)
    usable = (doc_pos == last_in) & (empty_in < 0.5)
    carried = jnp.where(usable, cum + top_in, far_low)
    peak = jnp.maximum(carried, lax.optimization_barrier(jnp.max(exponent, axis=1)))
    scores = jnp.einsum('td,sd->ts', queries_blk.astype(jnp.float32), keys_blk.astype(jnp.float32)) * scale
    weights = jnp.where(keep, scores * jnp.exp(exponent - peak[:, None]), 0.0)
    inter = jnp.where(usable, jnp.exp(carried - peak), 0.0)
    query_wide = queries_blk.astype(jnp.float32)
    numer = jnp.dot(weights.astype(jnp.bfloat16), values_blk, preferred_element_type=jnp.float32)
    numer = numer + (inter * scale)[:, None] * jnp.dot(query_wide, memory, precision=lax.Precision.HIGHEST)
    denom = lax.optimization_barrier(jnp.sum(weights, axis=1)) + inter * scale * jnp.dot(query_wide, norm_keys, precision=lax.Precision.HIGHEST)
    return numer / jnp.maximum(jnp.abs(denom), 1.0)[:, None]

def combine(early, late):
    e_mem, e_keys, e_top, e_total, e_first, e_last, e_empty = early
    l_mem, l_keys, l_top, l_total, l_first, l_last, l_empty = late
    linked = (l_first == e_last) & (l_first == l_last) & (e_empty < 0.5)
    top = jnp.where(linked, jnp.maximum(l_top, e_top + l_total), l_top)
    early_part = jnp.where(linked, jnp.exp(jnp.minimum(e_top + l_total - top, 0.0)), 0.0)
    late_part = jnp.exp(l_top - top)
    joined = (early_part * e_mem + late_part * l_mem, early_part * e_keys + late_part * l_keys, top, e_total + l_total, jnp.where(e_empty > 0.5, l_first, e_first), l_last, jnp.zeros_like(l_empty))
    return tuple((jnp.where(l_empty > 0.5, a, b) for a, b in zip(early, joined)))

def run_direction(queries_h, keys_h, values_h, in_gate, forget_pre, doc_pos):

    def blocks(arr):
        return arr.reshape((N_SP, TOK_DEV) + arr.shape[1:])

    def step(state, pieces):
        q_blk, k_blk, v_blk, i_blk, f_blk, d_blk = pieces
        result = emit(q_blk, k_blk, v_blk, i_blk, f_blk, d_blk, state)
        return (combine(state, summarize(k_blk, v_blk, i_blk, f_blk, d_blk)), result)
    start = (jnp.zeros((DQK, DV), jnp.float32), jnp.zeros((DQK,), jnp.float32), jnp.full((), far_low, jnp.float32), jnp.zeros((), jnp.float32), jnp.full((), -1.0, jnp.float32), jnp.full((), -1.0, jnp.float32), jnp.ones((), jnp.float32))
    final, results = lax.scan(step, start, (blocks(queries_h), blocks(keys_h), blocks(values_h), blocks(in_gate), blocks(forget_pre), blocks(doc_pos)))
    return results.reshape(TOKENS, DV)

def reference(queries, keys, values, out_gate, input_gates, forget_gates, doc_ids, head_gain, w_out, resid, norm_gain, w_up, w_down):
    doc_pos = doc_ids.astype(jnp.float32)
    summed = jnp.zeros((TOKENS, D), jnp.float32)
    for head in range(HEADS):
        q_head = queries[:, head * DQK:(head + 1) * DQK]
        k_head = keys[:, head * DQK:(head + 1) * DQK]
        v_head = values[:, head * DV:(head + 1) * DV]
        forward = run_direction(q_head, k_head, v_head, input_gates[0, head], forget_gates[0, head], doc_pos)
        backward = run_direction(q_head[::-1], k_head[::-1], v_head[::-1], input_gates[1, head, ::-1], forget_gates[1, head, ::-1], doc_pos[::-1])[::-1]
        memory = forward + backward
        normed = memory * lax.rsqrt(lax.optimization_barrier(jnp.mean(memory * memory, axis=-1, keepdims=True)) + eps)
        gate = jax.nn.sigmoid(out_gate[:, head * DV:(head + 1) * DV].astype(jnp.float32))
        readout = (normed * head_gain[head * DV:(head + 1) * DV] * gate).astype(jnp.bfloat16)
        part = jnp.dot(readout, w_out[head * DV:(head + 1) * DV], preferred_element_type=jnp.float32).astype(jnp.bfloat16)
        summed = summed + lax.optimization_barrier(part).astype(jnp.float32)
    mixed = resid.astype(jnp.float32) + summed
    scaled = (mixed * lax.rsqrt(lax.optimization_barrier(jnp.mean(mixed * mixed, axis=-1, keepdims=True)) + eps) * norm_gain).astype(jnp.bfloat16)
    width = FF // HEADS

    def feed(rows_blk):
        hidden = jnp.square(jax.nn.relu(jnp.dot(rows_blk, w_up, preferred_element_type=jnp.float32))).astype(jnp.bfloat16)
        total = jnp.zeros((rows_blk.shape[0], D), jnp.float32)
        for group in range(HEADS):
            part = jnp.dot(hidden[:, group * width:(group + 1) * width], w_down[group * width:(group + 1) * width], preferred_element_type=jnp.float32).astype(jnp.bfloat16)
            total = total + lax.optimization_barrier(part).astype(jnp.float32)
        return total
    mixer = lax.map(feed, scaled.reshape(N_SP, TOK_DEV, D)).reshape(TOKENS, D)
    return (mixed + mixer).astype(jnp.bfloat16)
```

```python
import jax
import jax.numpy as jnp
from jax import lax
from jax.experimental import pallas as pl
from jax.experimental.pallas import tpu as pltpu
from jax.sharding import PartitionSpec as P

EPS = 1e-06
FAR_LOW = -1e30
LONGEST_DOC = 3072
EXTRA = 128


def pair_of(count):
    return 2 if count % 2 == 0 else 1


def inner_flip(value, axis):
    count = lax.axis_size(axis)
    return lax.ppermute(value, axis, [(i, i ^ 1) for i in range(count)])


def outer_shift(value, axis, step, flip=0):
    count = lax.axis_size(axis)
    inner = pair_of(count)
    outer = count // inner
    moves = []
    for a in range(outer):
        for c in range(inner):
            moves.append((a * inner + c, ((a + step) % outer) * inner + (c ^ flip)))
    return lax.ppermute(value, axis, moves)


def line_shift(value, axis, step):
    count = lax.axis_size(axis)
    return lax.ppermute(
        value, axis, [(b, b + step) for b in range(count) if 0 <= b + step < count]
    )


def running_sums(rows):
    length = rows.shape[1]
    lane = lax.broadcasted_iota(jnp.int32, rows.shape, 1)
    left, right = rows, rows
    step = 1
    while step < length:
        left = left + jnp.where(lane >= step, pltpu.roll(left, step, 1), 0.0)
        right = right + jnp.where(lane < length - step, pltpu.roll(right, length - step, 1), 0.0)
        step *= 2
    return left, right


def log_sigmoid(x):
    return jnp.minimum(x, 0.0) - jnp.log1p(jnp.exp(-jnp.abs(x)))


def three_parts(x):
    high = x.astype(jnp.bfloat16).astype(jnp.float32)
    rest = x - high
    mid = rest.astype(jnp.bfloat16).astype(jnp.float32)
    return high, mid, rest - mid


def summary_kernel(keys, values, gates, out_f, out_b):
    dqk = keys.shape[1]
    dv = values.shape[1]
    length = keys.shape[0]
    rows = gates[...]
    left, right = running_sums(log_sigmoid(rows))
    doc = rows[4:5]
    first, last = doc[:, :1], doc[:, length - 1 :]
    keys_t = keys[...].astype(jnp.float32).T
    vals = values[...]
    lane = lax.broadcasted_iota(jnp.int32, (dqk, EXTRA), 1)
    for cum, total, in_gate, edge, out in (
        (left[2:3], left[2:3, length - 1 :], rows[0:1], last, out_f),
        (right[3:4], right[3:4, :1], rows[1:2], first, out_b),
    ):
        exponent = jnp.where(doc == edge, total - cum + in_gate, FAR_LOW)
        peak = jnp.max(exponent, axis=1, keepdims=True)
        weighted = (keys_t * jnp.exp(exponent - peak)).astype(jnp.bfloat16)
        out[:, :dv] = jnp.dot(weighted, vals, preferred_element_type=jnp.float32).astype(
            jnp.bfloat16
        )
        sums = jnp.sum(weighted.astype(jnp.float32), axis=1, keepdims=True)
        high = sums.astype(jnp.bfloat16).astype(jnp.float32)
        side = jnp.where(lane == 0, high, jnp.where(lane == 1, sums - high, 0.0))
        for at, part in enumerate(three_parts(peak) + three_parts(total) + (edge,)):
            side = jnp.where(lane == 2 + at, part, side)
        out[:, dv:] = side.astype(jnp.bfloat16)


def summaries(keys, values, gates):
    shape = jax.ShapeDtypeStruct((keys.shape[1], values.shape[1] + EXTRA), jnp.bfloat16)
    return pl.pallas_call(summary_kernel, out_shape=(shape, shape), name="summary")(
        keys, values, gates
    )


def emit_kernel(reach, place, queries, keys, values, gates, out_gate, gain, *rest):
    states_f, states_b = rest[:reach], rest[reach : 2 * reach]
    readout, row_buf, col_buf, carry_hi, carry_lo, top_buf = rest[2 * reach :]
    length, dv = values.shape
    tile = queries.shape[0]
    step = pl.program_id(0)
    scale = queries.shape[1] ** (-0.5)

    @pl.when(step == 0)
    def _():
        rows = gates[...]
        left, right = running_sums(log_sigmoid(rows))
        doc = rows[4:5]
        pack = jnp.concatenate(
            [left[2:3], right[3:4], rows[0:1] - left[2:3], rows[1:2] - right[3:4], doc, doc, doc, doc],
            axis=0,
        )
        row_buf[...] = pack
        col_buf[...] = pack.T
        for way, states in enumerate((states_f, states_b)):
            between = jnp.zeros((1, 1), jnp.float32)
            wanted = None
            heights, linked = [], []
            for j, state in enumerate(states):
                side = state[:16, dv:].astype(jnp.float32)[:1]
                peak = side[:, 2:3] + side[:, 3:4] + side[:, 4:5]
                total = side[:, 5:6] + side[:, 6:7] + side[:, 7:8]
                edge = side[:, 8:9]
                there = place[way] > j
                wanted = edge if j == 0 else wanted
                link = jnp.logical_and(edge == wanted, there)
                heights.append(jnp.where(link, peak + between, FAR_LOW))
                linked.append(link)
                between = between + total
            top = heights[0]
            for height in heights[1:]:
                top = jnp.maximum(top, height)
            carry = None
            for state, height, link in zip(states, heights, linked):
                part = jnp.where(link, jnp.exp(height - top), 0.0) * state[...].astype(jnp.float32)
                carry = part if carry is None else carry + part
            high = carry.astype(jnp.bfloat16)
            carry_hi[way] = high
            carry_lo[way] = (carry - high.astype(jnp.float32)).astype(jnp.bfloat16)
            top_buf[way] = jnp.broadcast_to(
                jnp.concatenate([top, jnp.where(linked[0], wanted, -1.0)], axis=0), (2, 128)
            )

    query = queries[...]
    scores = (
        lax.dot_general(
            query, keys[...], (((1,), (1,)), ((), ())), preferred_element_type=jnp.float32
        )
        * scale
    )
    cols = col_buf[pl.ds(step * tile, tile), :]
    rows = row_buf[...]
    at_t = step * tile + lax.broadcasted_iota(jnp.int32, scores.shape, 0)
    at_s = lax.broadcasted_iota(jnp.int32, scores.shape, 1)
    same = cols[:, 4:5] == rows[4:5]
    mixed = None
    memory = None
    for way in range(2):
        order = at_t >= at_s if way == 0 else at_t <= at_s
        keep = jnp.logical_and(order, same)
        cum = cols[:, way : way + 1]
        inside = rows[2 + way : 3 + way]
        usable = cols[:, 4:5] == top_buf[way, 1:2, :1]
        carried = jnp.where(usable, cum + top_buf[way, :1, :1], FAR_LOW)
        peak = jnp.maximum(
            carried, cum + jnp.max(jnp.where(keep, inside, FAR_LOW), axis=1, keepdims=True)
        )
        weights = jnp.where(keep, scores * jnp.exp(inside + (cum - peak)), 0.0)
        inter = jnp.where(usable, jnp.exp(carried - peak), 0.0) * scale
        got = jnp.dot(query, carry_hi[way], preferred_element_type=jnp.float32) + jnp.dot(
            query, carry_lo[way], preferred_element_type=jnp.float32
        )
        denom = jnp.sum(weights, axis=1, keepdims=True) + inter * (
            got[:, dv : dv + 1] + got[:, dv + 1 : dv + 2]
        )
        share = 1.0 / jnp.maximum(jnp.abs(denom), 1.0)
        part = weights * share
        mixed = part if mixed is None else mixed + part
        part = got[:, :dv] * (inter * share)
        memory = part if memory is None else memory + part
    memory = memory + jnp.dot(
        mixed.astype(jnp.bfloat16), values[...], preferred_element_type=jnp.float32
    )
    factor = lax.rsqrt(jnp.mean(memory * memory, axis=1, keepdims=True) + EPS)
    gate = 1.0 / (1.0 + jnp.exp(-out_gate[...].astype(jnp.float32)))
    readout[...] = (memory * factor * gain[...] * gate).astype(jnp.bfloat16)


def emit(place, queries, keys, values, gates, out_gate, gain, states_f, states_b):
    length, dqk = queries.shape
    dv = values.shape[1]
    tile = length // 3 if length % 384 == 0 else length
    reach = len(states_f)
    whole = lambda a: pl.BlockSpec(a.shape, lambda i, *_: (0,) * a.ndim)
    by_rows = lambda width: pl.BlockSpec((tile, width), lambda i, *_: (i, 0))
    import functools

    return pl.pallas_call(
        functools.partial(emit_kernel, reach),
        out_shape=jax.ShapeDtypeStruct((length, dv), jnp.bfloat16),
        grid_spec=pltpu.PrefetchScalarGridSpec(
            num_scalar_prefetch=1,
            grid=(length // tile,),
            in_specs=[
                by_rows(dqk),
                whole(keys),
                whole(values),
                whole(gates),
                by_rows(dv),
                whole(gain),
            ]
            + [whole(s) for s in (*states_f, *states_b)],
            out_specs=by_rows(dv),
            scratch_shapes=[
                pltpu.VMEM((8, length), jnp.float32),
                pltpu.VMEM((length, 8), jnp.float32),
                pltpu.VMEM((2, dqk, dv + EXTRA), jnp.bfloat16),
                pltpu.VMEM((2, dqk, dv + EXTRA), jnp.bfloat16),
                pltpu.VMEM((2, 2, 128), jnp.float32),
            ],
        ),
        name="emit",
    )(place, queries, keys, values, gates, out_gate, gain, *states_f, *states_b)


def project_kernel(count, *refs):
    pieces, weights = refs[:count], refs[count : 2 * count]
    resid, gain, mixed_out, normed_out = refs[2 * count :]
    mixed = resid[...].astype(jnp.float32)
    for piece, weight in zip(pieces, weights):
        mixed = mixed + jnp.dot(piece[...], weight[...], preferred_element_type=jnp.float32)
    mixed_out[...] = mixed
    factor = lax.rsqrt(jnp.mean(mixed * mixed, axis=1, keepdims=True) + EPS)
    normed_out[...] = (mixed * factor * gain[...]).astype(jnp.bfloat16)


def project(pieces, weights, resid, gain):
    import functools

    return pl.pallas_call(
        functools.partial(project_kernel, len(pieces)),
        out_shape=(
            jax.ShapeDtypeStruct(resid.shape, jnp.float32),
            jax.ShapeDtypeStruct(resid.shape, jnp.bfloat16),
        ),
        name="project",
    )(*pieces, *weights, resid, gain)


def tp_everywhere(value):
    count = lax.axis_size("tp")
    inner = pair_of(count)
    got = []
    for step in range(count // inner):
        here = value if step == 0 else outer_shift(value, "tp", step)
        got.append(here)
        if inner == 2:
            got.append(inner_flip(here, "tp"))
    return got


def tp_exchange(value):
    count = lax.axis_size("tp")
    inner = pair_of(count)
    outer = count // inner
    place = lax.axis_index("tp")
    a, c = place // inner, place % inner
    rows = value.shape[0] // count
    got = []
    for step in range(outer):
        for flip in range(inner):
            to = ((a + step) % outer) * inner + (c ^ flip)
            block = lax.dynamic_slice_in_dim(value, to * rows, rows, 0)
            got.append(block if step == flip == 0 else outer_shift(block, "tp", step, flip))
    return got


def tp_sum_back(parts, rows):
    count = lax.axis_size("tp")
    inner = pair_of(count)
    outer = count // inner
    total = None
    for step in range(outer):
        block = parts[step * inner * rows : (step + 1) * inner * rows]
        mine = block[:rows].astype(jnp.float32)
        if inner == 2:
            mine = mine + inner_flip(block[rows:], "tp").astype(jnp.float32)
        if step:
            mine = outer_shift(mine.astype(jnp.bfloat16), "tp", outer - step).astype(jnp.float32)
        total = mine if total is None else total + mine
    return total


def ring_shards(shard):
    count = lax.axis_size("sp")
    inner = pair_of(count)
    outer = count // inner
    got = []
    here = shard
    for step in range(outer):
        if step:
            here = outer_shift(here, "sp", 1)
        got.append((here, inner_flip(here, "sp")) if inner == 2 else (here,))
    return got


def ring_source(step, flip):
    count = lax.axis_size("sp")
    inner = pair_of(count)
    outer = count // inner
    place = lax.axis_index("sp")
    return ((place // inner - step) % outer) * inner + ((place % inner) ^ flip)


def shards(
    queries,
    keys,
    values,
    out_gate,
    input_gates,
    forget_gates,
    doc_ids,
    head_gain,
    w_out,
    resid,
    norm_gain,
    w_up,
    w_down,
):
    length = queries.shape[0]
    heads = input_gates.shape[1]
    blocks = lax.axis_size("sp")
    block = lax.axis_index("sp")
    up_ring = ring_shards(w_up)
    down_ring = ring_shards(w_down)
    out_shards = tp_everywhere(w_out)

    reach = min(blocks - 1, -(-(LONGEST_DOC - 1) // length))
    doc_pos = doc_ids.astype(jnp.float32)[None]
    place = jnp.stack([block, blocks - 1 - block]).astype(jnp.int32)
    readouts = []
    for h in range(heads):
        cut = lambda a: a.reshape(length, heads, -1)[:, h]
        k, v = cut(keys), cut(values)
        gates = jnp.concatenate(
            [input_gates[:, h], forget_gates[:, h], doc_pos, jnp.zeros((3, length), jnp.float32)]
        )
        sum_f, sum_b = summaries(k, v, gates)
        states_f = [line_shift(sum_f, "sp", j) for j in range(1, reach + 1)]
        states_b = [line_shift(sum_b, "sp", -j) for j in range(1, reach + 1)]
        readouts.append(
            emit(
                place,
                cut(queries),
                k,
                v,
                gates,
                cut(out_gate),
                head_gain.reshape(heads, 1, -1)[h],
                states_f,
                states_b,
            )
        )
    readout = readouts[0] if heads == 1 else jnp.concatenate(readouts, axis=1)
    mixed, normed = project(tp_exchange(readout), out_shards, resid, norm_gain[None])

    rows = normed.shape[0]
    gathered = jnp.concatenate(tp_everywhere(normed), axis=0)

    depth = w_up.shape[0]
    up_full = jnp.zeros((depth * blocks, w_up.shape[1]), w_up.dtype)
    for step, group in enumerate(up_ring):
        for flip, shard in enumerate(group):
            up_full = lax.dynamic_update_slice_in_dim(
                up_full, shard, ring_source(step, flip) * depth, 0
            )
    hidden = jnp.square(
        jax.nn.relu(jnp.dot(gathered, up_full, preferred_element_type=jnp.float32))
    ).astype(jnp.bfloat16)

    width = w_down.shape[1]
    out = jnp.zeros(resid.shape, jnp.bfloat16)
    for step, group in enumerate(down_ring):
        parts = jnp.concatenate(
            [
                jnp.dot(hidden, shard, preferred_element_type=jnp.float32).astype(jnp.bfloat16)
                for shard in group
            ],
            axis=1,
        )
        summed = tp_sum_back(parts, rows)
        for flip in range(len(group)):
            start = ring_source(step, flip) * width
            piece = summed[:, flip * width : (flip + 1) * width]
            base = lax.dynamic_slice_in_dim(mixed, start, width, 1)
            out = lax.dynamic_update_slice_in_dim(
                out, (base + piece).astype(jnp.bfloat16), start, 1
            )
    return out


def solution(mesh):
    in_specs = (
        P("sp", "tp"),
        P("sp", "tp"),
        P("sp", "tp"),
        P("sp", "tp"),
        P(None, "tp", "sp"),
        P(None, "tp", "sp"),
        P("sp"),
        P("tp"),
        P("tp", None),
        P(("sp", "tp"), None),
        P(),
        P("sp", "tp"),
        P("tp", "sp"),
    )
    out_specs = P(("sp", "tp"), None)
    return jax.shard_map(shards, mesh=mesh, in_specs=in_specs, out_specs=out_specs, check_vma=False)
```

```python
import functools

import jax
import jax.numpy as jnp
from jax import lax
from jax.experimental import pallas as pl
from jax.experimental.pallas import tpu as pltpu
from jax.sharding import PartitionSpec as P

EPS = 1e-06
FAR_LOW = -1e30
LONGEST_DOC = 3072
EXTRA = 128


def places(axis):
    outer = lax.axis_size(axis) // 2
    assert outer * 2 == lax.axis_size(axis)
    index = lax.axis_index(axis)
    return outer, index // 2, index % 2


def flip(value, axis):
    return lax.ppermute(value, axis, [(i, i ^ 1) for i in range(lax.axis_size(axis))])


def shift(value, axis, step, cross=0):
    outer = lax.axis_size(axis) // 2
    moves = [
        (2 * a + c, 2 * ((a + step) % outer) + (c ^ cross)) for a in range(outer) for c in range(2)
    ]
    return lax.ppermute(value, axis, moves)


def carry_shift(value, step):
    outer = lax.axis_size("sp") // 2
    moves = [(2 * a, 2 * (a - step)) for a in range(step, outer)]
    moves += [(2 * a + 1, 2 * (a + step) + 1) for a in range(outer - step)]
    return lax.ppermute(value, "sp", moves)


def running_sums(rows):
    length = rows.shape[1]
    lane = lax.broadcasted_iota(jnp.int32, rows.shape, 1)
    left, right = rows, rows
    step = 1
    while step < length:
        left = left + jnp.where(lane >= step, pltpu.roll(left, step, 1), 0.0)
        right = right + jnp.where(lane < length - step, pltpu.roll(right, length - step, 1), 0.0)
        step *= 2
    return left, right


def log_sigmoid(x):
    return jnp.minimum(x, 0.0) - jnp.log1p(jnp.exp(-jnp.abs(x)))


def three_parts(x):
    high = x.astype(jnp.bfloat16).astype(jnp.float32)
    rest = x - high
    mid = rest.astype(jnp.bfloat16).astype(jnp.float32)
    return high, mid, rest - mid


def pack_side(sums, peak, total, edge, shape):
    lane = lax.broadcasted_iota(jnp.int32, shape, 1)
    high = sums.astype(jnp.bfloat16).astype(jnp.float32)
    side = jnp.where(lane == 0, high, jnp.where(lane == 1, sums - high, 0.0))
    for at, part in enumerate(three_parts(peak) + three_parts(total) + (edge,)):
        side = jnp.where(lane == 2 + at, part, side)
    return side.astype(jnp.bfloat16)


def merge(states, valid, dv):
    between = jnp.zeros((1, 1), jnp.float32)
    heights, links = [], []
    for state, there in zip(states, valid):
        side = state[:16, dv:].astype(jnp.float32)[:1]
        peak = side[:, 2:3] + side[:, 3:4] + side[:, 4:5]
        total = side[:, 5:6] + side[:, 6:7] + side[:, 7:8]
        edge = side[:, 8:9]
        wanted = wanted if links else edge
        link = jnp.logical_and(edge == wanted, edge >= 0.0)
        if there is not None:
            link = jnp.logical_and(link, there)
        heights.append(jnp.where(link, peak + between, FAR_LOW))
        links.append(link)
        between = between + total
    top = heights[0]
    for height in heights[1:]:
        top = jnp.maximum(top, height)
    carry = None
    for state, height, link in zip(states, heights, links):
        part = jnp.where(link, jnp.exp(height - top), 0.0) * state[...].astype(jnp.float32)
        carry = part if carry is None else carry + part
    return carry, top, between, jnp.where(links[0], wanted, -1.0)


def put_state(out, carry, top, total, edge, dv):
    out[:, :dv] = carry[:, :dv].astype(jnp.bfloat16)
    sums = carry[:, dv : dv + 1] + carry[:, dv + 1 : dv + 2]
    out[:, dv:] = pack_side(sums, top, total, edge, (carry.shape[0], EXTRA))


def summary_kernel(info, keys, values, gates, give, mine):
    dqk = keys.shape[1]
    dv = values.shape[1]
    length = keys.shape[0]
    rows = gates[...]
    left, right = running_sums(log_sigmoid(rows))
    doc = rows[4:5]
    first, last = doc[:, :1], doc[:, length - 1 :]
    keys_t = keys[...].astype(jnp.float32).T
    vals = values[...]
    upper = info[0] == 1
    for cum, total, in_gate, edge, holder in (
        (left[2:3], left[2:3, length - 1 :], rows[0:1], last, upper),
        (right[3:4], right[3:4, :1], rows[1:2], first, jnp.logical_not(upper)),
    ):
        exponent = jnp.where(doc == edge, total - cum + in_gate, FAR_LOW)
        peak = jnp.max(exponent, axis=1, keepdims=True)
        weighted = (keys_t * jnp.exp(exponent - peak)).astype(jnp.bfloat16)
        memory = jnp.dot(weighted, vals, preferred_element_type=jnp.float32).astype(jnp.bfloat16)
        sums = jnp.sum(weighted.astype(jnp.float32), axis=1, keepdims=True)
        side = pack_side(sums, peak, total, edge, (dqk, EXTRA))

        @pl.when(holder)
        def _():
            mine[:, :dv] = memory
            mine[:, dv:] = side

        @pl.when(jnp.logical_not(holder))
        def _():
            give[:, :dv] = memory
            give[:, dv:] = side


SMALL = pl.BlockSpec(memory_space=pltpu.SMEM)
LOCAL = pl.BlockSpec(memory_space=pltpu.VMEM)


def summaries(info, keys, values, gates):
    shape = jax.ShapeDtypeStruct((keys.shape[1], values.shape[1] + EXTRA), jnp.bfloat16)
    return pl.pallas_call(
        summary_kernel,
        out_shape=(shape, shape),
        in_specs=[SMALL, LOCAL, LOCAL, LOCAL],
        name="summary",
    )(info, keys, values, gates)


def pair_kernel(mine, got, out):
    dv = mine.shape[1] - EXTRA
    put_state(out, *merge((mine, got), (None, None), dv), dv)


def pair_state(mine, got):
    return pl.pallas_call(
        pair_kernel, out_shape=jax.ShapeDtypeStruct(mine.shape, mine.dtype), name="pair"
    )(mine, got)


def lead_kernel(info, *refs):
    states, out = refs[:-1], refs[-1]
    dv = out.shape[1] - EXTRA
    valid = [info[1] > j for j in range(len(states))]
    put_state(out, *merge(states, valid, dv), dv)


def lead_state(info, states):
    return pl.pallas_call(
        lead_kernel,
        out_shape=jax.ShapeDtypeStruct(states[0].shape, states[0].dtype),
        in_specs=[SMALL] + [LOCAL] * len(states),
        name="lead",
    )(info, *states)


def emit_kernel(reach, info, queries, keys, values, gates, out_gate, gain, *rest):
    states, handed = rest[: reach + 1], rest[reach + 1]
    readout, row_buf, col_buf, carry_hi, carry_lo, top_buf = rest[reach + 2 :]
    _, dv = values.shape
    tile = queries.shape[0]
    step = pl.program_id(0)
    scale = queries.shape[1] ** (-0.5)

    @pl.when(step == 0)
    def _():
        rows = gates[...]
        left, right = running_sums(log_sigmoid(rows))
        doc = rows[4:5]
        cums = [left[2:3], right[3:4], rows[0:1] - left[2:3], rows[1:2] - right[3:4]]
        pack = jnp.concatenate(cums + [doc] * 4, axis=0)
        row_buf[...] = pack
        col_buf[...] = pack.T
        valid = [None] + [info[1] > j for j in range(reach)]
        held = 1 - info[0]
        for way, got, there in ((held, states, valid), (info[0], (handed,), (None,))):
            carry, top, _, edge = merge(got, there, dv)
            high = carry.astype(jnp.bfloat16)
            carry_hi[way] = high
            carry_lo[way] = (carry - high.astype(jnp.float32)).astype(jnp.bfloat16)
            top_buf[way] = jnp.broadcast_to(jnp.concatenate([top, edge], axis=0), (2, 128))

    query = queries[...]
    scores = (
        lax.dot_general(
            query, keys[...], (((1,), (1,)), ((), ())), preferred_element_type=jnp.float32
        )
        * scale
    )
    cols = col_buf[pl.ds(step * tile, tile), :]
    rows = row_buf[...]
    at_t = step * tile + lax.broadcasted_iota(jnp.int32, scores.shape, 0)
    at_s = lax.broadcasted_iota(jnp.int32, scores.shape, 1)
    same = cols[:, 4:5] == rows[4:5]
    mixed = None
    memory = None
    for way in range(2):
        order = at_t >= at_s if way == 0 else at_t <= at_s
        keep = jnp.logical_and(order, same)
        cum = cols[:, way : way + 1]
        inside = rows[2 + way : 3 + way]
        usable = cols[:, 4:5] == top_buf[way, 1:2, :1]
        carried = jnp.where(usable, cum + top_buf[way, :1, :1], FAR_LOW)
        peak = jnp.maximum(
            carried, cum + jnp.max(jnp.where(keep, inside, FAR_LOW), axis=1, keepdims=True)
        )
        weights = jnp.where(keep, scores * jnp.exp(inside + (cum - peak)), 0.0)
        inter = jnp.where(usable, jnp.exp(carried - peak), 0.0) * scale
        got = jnp.dot(query, carry_hi[way], preferred_element_type=jnp.float32) + jnp.dot(
            query, carry_lo[way], preferred_element_type=jnp.float32
        )
        denom = jnp.sum(weights, axis=1, keepdims=True) + inter * (
            got[:, dv : dv + 1] + got[:, dv + 1 : dv + 2]
        )
        share = 1.0 / jnp.maximum(jnp.abs(denom), 1.0)
        part = weights * share
        mixed = part if mixed is None else mixed + part
        part = got[:, :dv] * (inter * share)
        memory = part if memory is None else memory + part
    memory = memory + jnp.dot(
        mixed.astype(jnp.bfloat16), values[...], preferred_element_type=jnp.float32
    )
    factor = lax.rsqrt(jnp.mean(memory * memory, axis=1, keepdims=True) + EPS)
    gate = 1.0 / (1.0 + jnp.exp(-out_gate[...].astype(jnp.float32)))
    readout[...] = (memory * factor * gain[...] * gate).astype(jnp.bfloat16)


def emit(info, queries, keys, values, gates, out_gate, gain, states, handed):
    length, dqk = queries.shape
    dv = values.shape[1]
    tile = length // 3 if length % 384 == 0 else length
    whole = lambda a: pl.BlockSpec(a.shape, lambda i, *_: (0,) * a.ndim)
    by_rows = lambda width: pl.BlockSpec((tile, width), lambda i, *_: (i, 0))
    return pl.pallas_call(
        functools.partial(emit_kernel, len(states) - 1),
        out_shape=jax.ShapeDtypeStruct((length, dv), jnp.bfloat16),
        grid_spec=pltpu.PrefetchScalarGridSpec(
            num_scalar_prefetch=1,
            grid=(length // tile,),
            in_specs=[
                by_rows(dqk),
                whole(keys),
                whole(values),
                whole(gates),
                by_rows(dv),
                whole(gain),
            ]
            + [whole(s) for s in (*states, handed)],
            out_specs=by_rows(dv),
            scratch_shapes=[
                pltpu.VMEM((8, length), jnp.float32),
                pltpu.VMEM((length, 8), jnp.float32),
                pltpu.VMEM((2, dqk, dv + EXTRA), jnp.bfloat16),
                pltpu.VMEM((2, dqk, dv + EXTRA), jnp.bfloat16),
                pltpu.VMEM((2, 2, 128), jnp.float32),
            ],
        ),
        name="emit",
    )(info, queries, keys, values, gates, out_gate, gain, *states, handed)


def project_kernel(count, *refs):
    pieces, weights = refs[:count], refs[count : 2 * count]
    resid, gain, mixed_out, normed_out = refs[2 * count :]
    mixed = resid[...].astype(jnp.float32)
    for piece, weight in zip(pieces, weights):
        mixed = mixed + jnp.dot(piece[...], weight[...], preferred_element_type=jnp.float32)
    mixed_out[...] = mixed
    factor = lax.rsqrt(jnp.mean(mixed * mixed, axis=1, keepdims=True) + EPS)
    normed_out[...] = (mixed * factor * gain[...]).astype(jnp.bfloat16)


def project(pieces, weights, resid, gain):
    return pl.pallas_call(
        functools.partial(project_kernel, len(pieces)),
        out_shape=(
            jax.ShapeDtypeStruct(resid.shape, jnp.float32),
            jax.ShapeDtypeStruct(resid.shape, jnp.bfloat16),
        ),
        name="project",
    )(*pieces, *weights, resid, gain)


def up_kernel(count, *refs):
    near, far = refs[:2]
    pieces = refs[2 : 2 + count]
    out, buf, acc, sems = refs[2 + count :]
    rows = near.shape[0]
    depth = pieces[0].shape[0]
    half = count // 2
    copies = [pltpu.make_async_copy(pieces[k], buf.at[k], sems.at[k]) for k in range(count)]
    for copy in copies:
        copy.start()
    for part in range(2):
        for k in range(part * half, (part + 1) * half):
            copies[k].wait()
        weight = buf[part * half : (part + 1) * half].reshape(half * depth, -1)
        for at, source in enumerate((near, far)):
            here = jnp.dot(
                source[:, part * half * depth : (part + 1) * half * depth],
                weight,
                preferred_element_type=jnp.float32,
            )
            span = slice(at * rows, (at + 1) * rows)
            if part == 0:
                acc[span] = here
            else:
                out[span] = jnp.square(jnp.maximum(acc[span] + here, 0.0)).astype(jnp.bfloat16)


def up_product(near, far, pieces):
    count = len(pieces)
    depth, width = pieces[0].shape
    total = 2 * near.shape[0]
    return pl.pallas_call(
        functools.partial(up_kernel, count),
        out_shape=jax.ShapeDtypeStruct((total, width), jnp.bfloat16),
        in_specs=[LOCAL, LOCAL] + [pl.BlockSpec(memory_space=pl.ANY)] * count,
        scratch_shapes=[
            pltpu.VMEM((count, depth, width), jnp.bfloat16),
            pltpu.VMEM((total, width), jnp.float32),
            pltpu.SemaphoreType.DMA((count,)),
        ],
        name="up",
    )(near, far, *pieces)


def tp_exchange(value):
    outer, a, c = places("tp")
    rows = value.shape[0] // (2 * outer)
    got = []
    for step in range(outer):
        for cross in range(2):
            to = 2 * ((a + step) % outer) + (c ^ cross)
            block = lax.dynamic_slice_in_dim(value, to * rows, rows, 0)
            if step or cross:
                block = shift(block, "tp", step, cross)
            got.append(block)
    return got


def tp_weights(value):
    outer = places("tp")[0]
    got = []
    for step in range(outer):
        here = shift(value, "tp", step) if step else value
        got += [here, flip(here, "tp")]
    return got


def tp_gather(value):
    outer = places("tp")[0]
    near = [value] + [shift(value, "tp", step) for step in range(1, outer)]
    near = jnp.concatenate(near, axis=0)
    return near, flip(near, "tp")


def tp_sum_back(parts, rows):
    outer = places("tp")[0]
    split = outer * rows
    paired = parts[:split].astype(jnp.float32) + flip(parts[split:], "tp").astype(jnp.float32)
    total = paired[:rows]
    for step in range(1, outer):
        block = paired[step * rows : (step + 1) * rows].astype(jnp.bfloat16)
        total = total + shift(block, "tp", outer - step).astype(jnp.float32)
    return total


def ring_shards(shard, hand_on):
    outer = places("sp")[0]
    here, got = shard, []
    for step in range(outer):
        if step:
            here = shift(here, "sp", 1)
        if hand_on and step and step == outer - 1:
            there = shift(got[-1][1], "sp", 1)
        else:
            there = flip(here, "sp")
        got.append((here, there))
    return got


def ring_sources():
    outer, a, c = places("sp")
    return [2 * ((a - step) % outer) + (c ^ cross) for step in range(outer) for cross in range(2)]


def shards(
    queries,
    keys,
    values,
    out_gate,
    input_gates,
    forget_gates,
    doc_ids,
    head_gain,
    w_out,
    resid,
    norm_gain,
    w_up,
    w_down,
):
    length = queries.shape[0]
    heads = input_gates.shape[1]
    outer, a, c = places("sp")
    up_ring = ring_shards(w_up, False)
    down_ring = ring_shards(w_down, True)
    out_shards = tp_weights(w_out)

    reach = min(2 * outer - 1, -(-(LONGEST_DOC - 1) // length))
    hops = min(outer - 1, -(-reach // 2))
    doc_pos = doc_ids.astype(jnp.float32)[None]
    info = jnp.stack([c, jnp.where(c == 1, a, outer - 1 - a)]).astype(jnp.int32)
    readouts = []
    for h in range(heads):
        cut = lambda x: x.reshape(length, heads, -1)[:, h]
        k, v = cut(keys), cut(values)
        gates = jnp.concatenate(
            [input_gates[:, h], forget_gates[:, h], doc_pos, jnp.zeros((3, length), jnp.float32)]
        )
        give, mine = summaries(info, k, v, gates)
        got = flip(give, "sp")
        pair = pair_state(mine, got)
        ahead = [carry_shift(pair, j) for j in range(1, hops + 1)]
        handed = flip(lead_state(info, ahead), "sp")
        readouts.append(
            emit(
                info,
                cut(queries),
                k,
                v,
                gates,
                cut(out_gate),
                head_gain.reshape(heads, 1, -1)[h],
                [got] + ahead,
                handed,
            )
        )
    readout = readouts[0] if heads == 1 else jnp.concatenate(readouts, axis=1)
    mixed, normed = project(tp_exchange(readout), out_shards, resid, norm_gain[None])

    rows = normed.shape[0]
    depth = w_up.shape[0]
    sources = ring_sources()
    turned = jnp.concatenate(
        [lax.dynamic_slice_in_dim(normed, at * depth, depth, 1) for at in sources], axis=1
    )
    near, far = tp_gather(turned)
    hidden = up_product(near, far, [shard for group in up_ring for shard in group])

    width = w_down.shape[1]
    out = jnp.zeros(resid.shape, jnp.bfloat16)
    for step, group in enumerate(down_ring):
        parts = []
        for shard in group:
            part = jnp.dot(hidden, shard, preferred_element_type=jnp.float32)
            parts.append(part.astype(jnp.bfloat16))
        parts = jnp.concatenate(parts, axis=1)
        summed = tp_sum_back(parts, rows)
        for cross in range(2):
            start = sources[2 * step + cross] * width
            piece = summed[:, cross * width : (cross + 1) * width]
            base = lax.dynamic_slice_in_dim(mixed, start, width, 1)
            out = lax.dynamic_update_slice_in_dim(
                out, (base + piece).astype(jnp.bfloat16), start, 1
            )
    return out


def solution(mesh):
    in_specs = (
        P("sp", "tp"),
        P("sp", "tp"),
        P("sp", "tp"),
        P("sp", "tp"),
        P(None, "tp", "sp"),
        P(None, "tp", "sp"),
        P("sp"),
        P("tp"),
        P("tp", None),
        P(("sp", "tp"), None),
        P(),
        P("sp", "tp"),
        P("tp", "sp"),
    )
    out_specs = P(("sp", "tp"), None)

    return jax.shard_map(shards, mesh=mesh, in_specs=in_specs, out_specs=out_specs, check_vma=False)
```

```python
import functools

import jax
import jax.numpy as jnp
from jax import lax
from jax.experimental import pallas as pl
from jax.experimental.pallas import tpu as pltpu
from jax.sharding import PartitionSpec as P

EPS = 1e-06
FAR_LOW = -1e30
LONGEST_DOC = 3072
LANES = 128
EXTRA = LANES


def places(axis):
    outer = lax.axis_size(axis) // 2
    assert outer * 2 == lax.axis_size(axis)
    index = lax.axis_index(axis)
    return outer, index // 2, index % 2


def flip(value, axis):
    return lax.ppermute(value, axis, [(i, i ^ 1) for i in range(lax.axis_size(axis))])


def shift(value, axis, step, cross=0):
    outer = lax.axis_size(axis) // 2
    moves = [
        (2 * a + c, 2 * ((a + step) % outer) + (c ^ cross)) for a in range(outer) for c in range(2)
    ]
    return lax.ppermute(value, axis, moves)


def neighbour(value):
    moves = [(i, i ^ 2) for i in range(lax.axis_size("sp"))]
    return lax.ppermute(value, "sp", moves)


def carry_shift(value, step):
    outer = lax.axis_size("sp") // 2
    moves = [(2 * a, 2 * (a - step)) for a in range(step, outer)]
    moves += [(2 * a + 1, 2 * (a + step) + 1) for a in range(outer - step)]
    return lax.ppermute(value, "sp", moves)


def running_sums(rows):
    length = rows.shape[1]
    lane = lax.broadcasted_iota(jnp.int32, rows.shape, 1)
    left, right = rows, rows
    step = 1
    while step < length:
        left = left + jnp.where(lane >= step, pltpu.roll(left, step, 1), 0.0)
        right = right + jnp.where(lane < length - step, pltpu.roll(right, length - step, 1), 0.0)
        step *= 2
    return left, right


def log_sigmoid(x):
    return jnp.minimum(x, 0.0) - jnp.log1p(jnp.exp(-jnp.abs(x)))


def three_parts(x):
    high = x.astype(jnp.bfloat16).astype(jnp.float32)
    rest = x - high
    mid = rest.astype(jnp.bfloat16).astype(jnp.float32)
    return high, mid, rest - mid


def pack_side(sums, peak, total, edge, shape):
    lane = lax.broadcasted_iota(jnp.int32, shape, 1)
    high = sums.astype(jnp.bfloat16).astype(jnp.float32)
    side = jnp.where(lane == 0, high, jnp.where(lane == 1, sums - high, 0.0))
    for at, part in enumerate(three_parts(peak) + three_parts(total) + (edge,)):
        side = jnp.where(lane == 2 + at, part, side)
    return side.astype(jnp.bfloat16)


def merge(states, valid, dv):
    between = jnp.zeros((1, 1), jnp.float32)
    heights, links = [], []
    for state, there in zip(states, valid):
        side = state[:16, dv:].astype(jnp.float32)[:1]
        peak = side[:, 2:3] + side[:, 3:4] + side[:, 4:5]
        total = side[:, 5:6] + side[:, 6:7] + side[:, 7:8]
        edge = side[:, 8:9]
        wanted = wanted if links else edge
        link = jnp.logical_and(edge == wanted, edge >= 0.0)
        if there is not None:
            link = jnp.logical_and(link, there)
        heights.append(jnp.where(link, peak + between, FAR_LOW))
        links.append(link)
        between = between + total
    top = heights[0]
    for height in heights[1:]:
        top = jnp.maximum(top, height)
    carry = None
    for state, height, link in zip(states, heights, links):
        part = jnp.where(link, jnp.exp(height - top), 0.0) * state[...].astype(jnp.float32)
        carry = part if carry is None else carry + part
    return carry, top, between, jnp.where(links[0], wanted, -1.0)


def put_state(out, carry, top, total, edge, dv):
    out[:, :dv] = carry[:, :dv].astype(jnp.bfloat16)
    sums = carry[:, dv : dv + 1] + carry[:, dv + 1 : dv + 2]
    out[:, dv:] = pack_side(sums, top, total, edge, (carry.shape[0], EXTRA))


def summary_kernel(info, keys, values, gates, give, mine):
    dqk = keys.shape[1]
    dv = values.shape[1]
    length = keys.shape[0]
    rows = gates[...]
    left, right = running_sums(log_sigmoid(rows))
    doc = rows[4:5]
    first, last = doc[:, :1], doc[:, length - 1 :]
    keys_t = keys[...].astype(jnp.float32).T
    vals = values[...]
    upper = info[0] == 1
    for cum, total, in_gate, edge, holder in (
        (left[2:3], left[2:3, length - 1 :], rows[0:1], last, upper),
        (right[3:4], right[3:4, :1], rows[1:2], first, jnp.logical_not(upper)),
    ):
        exponent = jnp.where(doc == edge, total - cum + in_gate, FAR_LOW)
        peak = jnp.max(exponent, axis=1, keepdims=True)
        weighted = (keys_t * jnp.exp(exponent - peak)).astype(jnp.bfloat16)
        memory = jnp.dot(weighted, vals, preferred_element_type=jnp.float32).astype(jnp.bfloat16)
        sums = jnp.sum(weighted.astype(jnp.float32), axis=1, keepdims=True)
        side = pack_side(sums, peak, total, edge, (dqk, EXTRA))

        @pl.when(holder)
        def _():
            mine[:, :dv] = memory
            mine[:, dv:] = side

        @pl.when(jnp.logical_not(holder))
        def _():
            give[:, :dv] = memory
            give[:, dv:] = side


SMALL = pl.BlockSpec(memory_space=pltpu.SMEM)
LOCAL = pl.BlockSpec(memory_space=pltpu.VMEM)


def summaries(info, keys, values, gates):
    shape = jax.ShapeDtypeStruct((keys.shape[1], values.shape[1] + EXTRA), jnp.bfloat16)
    return pl.pallas_call(
        summary_kernel,
        out_shape=(shape, shape),
        in_specs=[SMALL, LOCAL, LOCAL, LOCAL],
        name="summary",
    )(info, keys, values, gates)


def pair_kernel(mine, got, out):
    dv = mine.shape[1] - EXTRA
    put_state(out, *merge((mine, got), (None, None), dv), dv)


def pair_state(mine, got):
    return pl.pallas_call(
        pair_kernel, out_shape=jax.ShapeDtypeStruct(mine.shape, mine.dtype), name="pair"
    )(mine, got)


def lead_kernel(info, *refs):
    states, out = refs[:-1], refs[-1]
    dv = out.shape[1] - EXTRA
    valid = [info[1] > j for j in range(len(states))]
    put_state(out, *merge(states, valid, dv), dv)


def lead_state(info, states):
    return pl.pallas_call(
        lead_kernel,
        out_shape=jax.ShapeDtypeStruct(states[0].shape, states[0].dtype),
        in_specs=[SMALL] + [LOCAL] * len(states),
        name="lead",
    )(info, *states)


def emit_kernel(reach, info, queries, keys, values, gates, out_gate, gain, *rest):
    states, handed = rest[: reach + 1], rest[reach + 1]
    readout, row_buf, col_buf, carry_hi, carry_lo, top_buf = rest[reach + 2 :]
    _, dv = values.shape
    tile = queries.shape[0]
    step = pl.program_id(0)
    scale = queries.shape[1] ** (-0.5)

    @pl.when(step == 0)
    def _():
        rows = gates[...]
        left, right = running_sums(log_sigmoid(rows))
        doc = rows[4:5]
        cums = [left[2:3], right[3:4], rows[0:1] - left[2:3], rows[1:2] - right[3:4]]
        pack = jnp.concatenate(cums + [doc] * 4, axis=0)
        row_buf[...] = pack
        col_buf[...] = pack.T
        valid = [None] + [info[1] > j for j in range(reach)]
        held = 1 - info[0]
        for way, got, there in ((held, states, valid), (info[0], (handed,), (None,))):
            carry, top, _, edge = merge(got, there, dv)
            high = carry.astype(jnp.bfloat16)
            carry_hi[way] = high
            carry_lo[way] = (carry - high.astype(jnp.float32)).astype(jnp.bfloat16)
            top_buf[way] = jnp.broadcast_to(jnp.concatenate([top, edge], axis=0), (2, 128))

    query = queries[...]
    scores = (
        lax.dot_general(
            query, keys[...], (((1,), (1,)), ((), ())), preferred_element_type=jnp.float32
        )
        * scale
    )
    cols = col_buf[pl.ds(step * tile, tile), :]
    rows = row_buf[...]
    at_t = step * tile + lax.broadcasted_iota(jnp.int32, scores.shape, 0)
    at_s = lax.broadcasted_iota(jnp.int32, scores.shape, 1)
    same = cols[:, 4:5] == rows[4:5]
    mixed = None
    memory = None
    for way in range(2):
        order = at_t >= at_s if way == 0 else at_t <= at_s
        keep = jnp.logical_and(order, same)
        cum = cols[:, way : way + 1]
        inside = rows[2 + way : 3 + way]
        usable = cols[:, 4:5] == top_buf[way, 1:2, :1]
        carried = jnp.where(usable, cum + top_buf[way, :1, :1], FAR_LOW)
        peak = jnp.maximum(
            carried, cum + jnp.max(jnp.where(keep, inside, FAR_LOW), axis=1, keepdims=True)
        )
        weights = jnp.where(keep, scores * jnp.exp(inside + (cum - peak)), 0.0)
        inter = jnp.where(usable, jnp.exp(carried - peak), 0.0) * scale
        got = jnp.dot(query, carry_hi[way], preferred_element_type=jnp.float32) + jnp.dot(
            query, carry_lo[way], preferred_element_type=jnp.float32
        )
        denom = jnp.sum(weights, axis=1, keepdims=True) + inter * (
            got[:, dv : dv + 1] + got[:, dv + 1 : dv + 2]
        )
        share = 1.0 / jnp.maximum(jnp.abs(denom), 1.0)
        part = weights * share
        mixed = part if mixed is None else mixed + part
        part = got[:, :dv] * (inter * share)
        memory = part if memory is None else memory + part
    memory = memory + jnp.dot(
        mixed.astype(jnp.bfloat16), values[...], preferred_element_type=jnp.float32
    )
    factor = lax.rsqrt(jnp.mean(memory * memory, axis=1, keepdims=True) + EPS)
    gate = 1.0 / (1.0 + jnp.exp(-out_gate[...].astype(jnp.float32)))
    readout[...] = (memory * factor * gain[...] * gate).astype(jnp.bfloat16)


def emit(info, queries, keys, values, gates, out_gate, gain, states, handed):
    length, dqk = queries.shape
    dv = values.shape[1]
    tile = length // 3 if length % 384 == 0 else length
    whole = lambda a: pl.BlockSpec(a.shape, lambda i, *_: (0,) * a.ndim)
    by_rows = lambda width: pl.BlockSpec((tile, width), lambda i, *_: (i, 0))
    return pl.pallas_call(
        functools.partial(emit_kernel, len(states) - 1),
        out_shape=jax.ShapeDtypeStruct((length, dv), jnp.bfloat16),
        grid_spec=pltpu.PrefetchScalarGridSpec(
            num_scalar_prefetch=1,
            grid=(length // tile,),
            in_specs=[
                by_rows(dqk),
                whole(keys),
                whole(values),
                whole(gates),
                by_rows(dv),
                whole(gain),
            ]
            + [whole(s) for s in (*states, handed)],
            out_specs=by_rows(dv),
            scratch_shapes=[
                pltpu.VMEM((8, length), jnp.float32),
                pltpu.VMEM((length, 8), jnp.float32),
                pltpu.VMEM((2, dqk, dv + EXTRA), jnp.bfloat16),
                pltpu.VMEM((2, dqk, dv + EXTRA), jnp.bfloat16),
                pltpu.VMEM((2, 2, 128), jnp.float32),
            ],
        ),
        name="emit",
    )(info, queries, keys, values, gates, out_gate, gain, *states, handed)


def project_kernel(count, turn, info, *refs):
    pieces, weights = refs[:count], refs[count : 2 * count]
    resid, gain, mixed_out, normed_out, beside_out, whole = refs[2 * count :]
    mixed = resid[...].astype(jnp.float32)
    for piece, weight in zip(pieces, weights):
        mixed = mixed + jnp.dot(piece[...], weight[...], preferred_element_type=jnp.float32)
    mixed_out[...] = mixed
    factor = lax.rsqrt(jnp.mean(mixed * mixed, axis=1, keepdims=True) + EPS)
    normed = mixed * factor * gain[...]
    if not turn:
        normed_out[...] = normed.astype(jnp.bfloat16)
        beside_out[...] = normed_out[...]
        return
    whole[...] = normed
    depth = mixed.shape[1] // turn
    for k in range(turn):
        at = pl.multiple_of(info[k] * depth, LANES)
        part = whole[:, pl.ds(at, depth)].astype(jnp.bfloat16)
        normed_out[:, k * depth : (k + 1) * depth] = part
        beside_out[:, (k ^ 1) * depth : ((k ^ 1) + 1) * depth] = part


def project(pieces, weights, resid, gain, sources, depth):
    inside = depth % LANES == 0
    mixed, normed, beside = pl.pallas_call(
        functools.partial(project_kernel, len(pieces), len(sources) if inside else 0),
        out_shape=(
            jax.ShapeDtypeStruct(resid.shape, jnp.float32),
            jax.ShapeDtypeStruct(resid.shape, jnp.bfloat16),
            jax.ShapeDtypeStruct(resid.shape, jnp.bfloat16),
        ),
        in_specs=[SMALL] + [LOCAL] * (2 * len(pieces) + 2),
        scratch_shapes=[pltpu.VMEM(resid.shape, jnp.float32)],
        name="project",
    )(jnp.stack(sources).astype(jnp.int32), *pieces, *weights, resid, gain)
    if not inside:
        cuts = [lax.dynamic_slice_in_dim(normed, at * depth, depth, 1) for at in sources]
        normed = jnp.concatenate(cuts, axis=1)
        beside = jnp.concatenate([cuts[k ^ 1] for k in range(len(cuts))], axis=1)
    return mixed, normed, beside


def up_kernel(blocks, count, *refs):
    rows = refs[:blocks]
    pieces = refs[blocks : blocks + count]
    out, buf, acc, sems = refs[blocks + count :]
    depth = pieces[0].shape[0]
    half = count // 2
    copies = [pltpu.make_async_copy(pieces[k], buf.at[k], sems.at[k]) for k in range(count)]
    for copy in copies:
        copy.start()
    for part in range(2):
        for k in range(part * half, (part + 1) * half):
            copies[k].wait()
        weight = buf[part * half : (part + 1) * half].reshape(half * depth, -1)
        at = 0
        for source in rows:
            here = jnp.dot(
                source[:, part * half * depth : (part + 1) * half * depth],
                weight,
                preferred_element_type=jnp.float32,
            )
            span = slice(at, at + source.shape[0])
            at += source.shape[0]
            if part == 0:
                acc[span] = here
            else:
                out[span] = jnp.square(jnp.maximum(acc[span] + here, 0.0)).astype(jnp.bfloat16)


def up_product(rows, pieces):
    count = len(pieces)
    depth, width = pieces[0].shape
    total = sum(r.shape[0] for r in rows)
    return pl.pallas_call(
        functools.partial(up_kernel, len(rows), count),
        out_shape=jax.ShapeDtypeStruct((total, width), jnp.bfloat16),
        in_specs=[LOCAL] * len(rows) + [pl.BlockSpec(memory_space=pl.ANY)] * count,
        scratch_shapes=[
            pltpu.VMEM((count, depth, width), jnp.bfloat16),
            pltpu.VMEM((total, width), jnp.float32),
            pltpu.SemaphoreType.DMA((count,)),
        ],
    )(*rows, *pieces)


def down_kernel(early, late, *refs):
    pieces, (near, far) = refs[:-2], refs[-2:]
    at = 0
    for piece in pieces:
        cols = slice(at, at + piece.shape[1])
        at += piece.shape[1]
        for place, out in enumerate((near, far)):
            top = 0
            for hidden in (early, late):
                rows = hidden.shape[0] // 2
                out[top : top + rows, cols] = jnp.dot(
                    hidden[place * rows : (place + 1) * rows],
                    piece[...],
                    preferred_element_type=jnp.float32,
                ).astype(jnp.bfloat16)
                top += rows


def down_product(early, late, pieces):
    rows = (early.shape[0] + late.shape[0]) // 2
    shape = jax.ShapeDtypeStruct((rows, sum(p.shape[1] for p in pieces)), jnp.bfloat16)
    return pl.pallas_call(down_kernel, out_shape=(shape, shape))(early, late, *pieces)


def tp_exchange(value):
    outer, a, c = places("tp")
    rows = value.shape[0] // (2 * outer)
    got = []
    for step in range(outer):
        for cross in range(2):
            to = 2 * ((a + step) % outer) + (c ^ cross)
            block = lax.dynamic_slice_in_dim(value, to * rows, rows, 0)
            if step or cross:
                block = shift(block, "tp", step, cross)
            got.append(block)
    return got


def tp_weights(value):
    outer = places("tp")[0]
    got = []
    for step in range(outer):
        here = shift(value, "tp", step) if step else value
        got += [here, flip(here, "tp")]
    return got


def row_blocks(value, given):
    outer = places("tp")[0]
    beside = neighbour(given)
    across = [shift(value, "tp", step) for step in range(1, outer)]
    late = [shift(beside, "tp", step) for step in range(1, outer)]
    second = jnp.concatenate([beside] + across, axis=0)
    third = late[0] if len(late) == 1 else jnp.concatenate(late, axis=0)
    return (value, second), (third,), (flip(value, "tp"), flip(second, "tp"), flip(third, "tp"))


def sum_back(near, far, rows, line_first):
    outer = places("tp")[0]
    paired = near.astype(jnp.float32) + flip(far, "tp").astype(jnp.float32)
    block = lambda k: paired[k * rows : (k + 1) * rows]
    send = lambda blocks: jnp.concatenate(blocks, axis=0).astype(jnp.bfloat16)
    own = [block(0)] + [block(1 + step) for step in range(1, outer)]
    beside = [block(1)] + [block(outer + step) for step in range(1, outer)]
    turned = lambda x: jnp.concatenate([x[:, x.shape[1] // 2 :], x[:, : x.shape[1] // 2]], axis=1)
    if line_first:
        got = neighbour(turned(send(beside))).astype(jnp.float32)
        own = [b + got[k * rows : (k + 1) * rows] for k, b in enumerate(own)]
        total = own[0]
        for step in range(1, outer):
            block_sent = own[step].astype(jnp.bfloat16)
            total = total + shift(block_sent, "tp", outer - step).astype(jnp.float32)
        return total
    total, other = own[0], beside[0]
    for step in range(1, outer):
        got = shift(send([own[step], beside[step]]), "tp", outer - step)
        total = total + got[:rows].astype(jnp.float32)
        other = other + got[rows:].astype(jnp.float32)
    other = turned(other.astype(jnp.bfloat16))
    return total + neighbour(other).astype(jnp.float32)


def half_shards(shard, dim):
    outer, a, _ = places("sp")
    size = shard.shape[dim] // 2
    kept = lax.dynamic_slice_in_dim(shard, (a % 2) * size, size, dim)
    given = lax.dynamic_slice_in_dim(shard, (1 - a % 2) * size, size, dim)
    here, got = [kept, neighbour(given)], []
    for step in range(outer // 2):
        if step:
            here = [shift(x, "sp", 2) for x in here]
        got += [here, [flip(x, "sp") for x in here]]
    return got


def ring_sources():
    outer, a, c = places("sp")
    assert outer % 2 == 0
    return [
        2 * (((a - 2 * step) % outer) ^ k) + (c ^ cross)
        for step in range(outer // 2)
        for cross in range(2)
        for k in range(2)
    ]


def shards(
    queries,
    keys,
    values,
    out_gate,
    input_gates,
    forget_gates,
    doc_ids,
    head_gain,
    w_out,
    resid,
    norm_gain,
    w_up,
    w_down,
):
    length = queries.shape[0]
    heads = input_gates.shape[1]
    outer, a, c = places("sp")
    up_ring = half_shards(w_up, 1)
    down_ring = half_shards(w_down, 0)
    out_shards = tp_weights(w_out)

    reach = min(2 * outer - 1, -(-(LONGEST_DOC - 1) // length))
    hops = min(outer - 1, -(-reach // 2))
    doc_pos = doc_ids.astype(jnp.float32)[None]
    info = jnp.stack([c, jnp.where(c == 1, a, outer - 1 - a)]).astype(jnp.int32)
    readouts = []
    for h in range(heads):
        cut = lambda x: x.reshape(length, heads, -1)[:, h]
        k, v = cut(keys), cut(values)
        gates = jnp.concatenate(
            [input_gates[:, h], forget_gates[:, h], doc_pos, jnp.zeros((3, length), jnp.float32)]
        )
        give, mine = summaries(info, k, v, gates)
        got = flip(give, "sp")
        pair = pair_state(mine, got)
        ahead = [carry_shift(pair, j) for j in range(1, hops + 1)]
        handed = flip(lead_state(info, ahead), "sp")
        readouts.append(
            emit(
                info,
                cut(queries),
                k,
                v,
                gates,
                cut(out_gate),
                head_gain.reshape(heads, 1, -1)[h],
                [got] + ahead,
                handed,
            )
        )
    readout = readouts[0] if heads == 1 else jnp.concatenate(readouts, axis=1)
    sources = ring_sources()
    mixed, normed, given = project(
        tp_exchange(readout), out_shards, resid, norm_gain[None], sources, w_up.shape[0]
    )
    rows = normed.shape[0]
    early, late, partner = row_blocks(normed, given)
    up_pieces = [shard for group in up_ring for shard in group]
    early = up_product([*early, *partner[:2]], up_pieces)
    late = up_product([*late, partner[2]], up_pieces)

    width = w_down.shape[1]
    out = jnp.zeros(resid.shape, jnp.bfloat16)
    for step, group in enumerate(down_ring):
        near, far = down_product(early, late, group)
        summed = sum_back(near, far, rows, step % 2 == 1)
        for k in range(2):
            start = sources[2 * step + k] * width
            piece = summed[:, k * width : (k + 1) * width]
            base = lax.dynamic_slice_in_dim(mixed, start, width, 1)
            out = lax.dynamic_update_slice_in_dim(
                out, (base + piece).astype(jnp.bfloat16), start, 1
            )
    return out


def solution(mesh):
    in_specs = (
        P("sp", "tp"),
        P("sp", "tp"),
        P("sp", "tp"),
        P("sp", "tp"),
        P(None, "tp", "sp"),
        P(None, "tp", "sp"),
        P("sp"),
        P("tp"),
        P("tp", None),
        P(("sp", "tp"), None),
        P(),
        P("sp", "tp"),
        P("tp", "sp"),
    )
    out_specs = P(("sp", "tp"), None)

    return jax.shard_map(shards, mesh=mesh, in_specs=in_specs, out_specs=out_specs, check_vma=False)
```

```python
import functools

import jax
import jax.numpy as jnp
from jax import lax
from jax.experimental import pallas as pl
from jax.experimental.pallas import tpu as pltpu
from jax.sharding import PartitionSpec as P

EPS = 1e-06
FAR_LOW = -1e30
LONGEST_DOC = 3072
LANES = 128
EXTRA = LANES


def places(axis):
    outer = lax.axis_size(axis) // 2
    assert outer * 2 == lax.axis_size(axis)
    index = lax.axis_index(axis)
    return outer, index // 2, index % 2


def flip(value, axis):
    return lax.ppermute(value, axis, [(i, i ^ 1) for i in range(lax.axis_size(axis))])


def shift(value, axis, step, cross=0):
    outer = lax.axis_size(axis) // 2
    moves = [
        (2 * a + c, 2 * ((a + step) % outer) + (c ^ cross)) for a in range(outer) for c in range(2)
    ]
    return lax.ppermute(value, axis, moves)


def neighbour(value):
    moves = [(i, i ^ 2) for i in range(lax.axis_size("sp"))]
    return lax.ppermute(value, "sp", moves)


def carry_shift(value, step):
    outer = lax.axis_size("sp") // 2
    moves = [(2 * a, 2 * (a - step)) for a in range(step, outer)]
    moves += [(2 * a + 1, 2 * (a + step) + 1) for a in range(outer - step)]
    return lax.ppermute(value, "sp", moves)


def running_sums(rows):
    length = rows.shape[1]
    lane = lax.broadcasted_iota(jnp.int32, rows.shape, 1)
    left, right = rows, rows
    step = 1
    while step < length:
        left = left + jnp.where(lane >= step, pltpu.roll(left, step, 1), 0.0)
        right = right + jnp.where(lane < length - step, pltpu.roll(right, length - step, 1), 0.0)
        step *= 2
    return left, right


def log_sigmoid(x):
    return jnp.minimum(x, 0.0) - jnp.log1p(jnp.exp(-jnp.abs(x)))


def three_parts(x):
    high = x.astype(jnp.bfloat16).astype(jnp.float32)
    rest = x - high
    mid = rest.astype(jnp.bfloat16).astype(jnp.float32)
    return high, mid, rest - mid


def pack_side(sums, peak, total, edge, shape):
    lane = lax.broadcasted_iota(jnp.int32, shape, 1)
    high = sums.astype(jnp.bfloat16).astype(jnp.float32)
    side = jnp.where(lane == 0, high, jnp.where(lane == 1, sums - high, 0.0))
    for at, part in enumerate(three_parts(peak) + three_parts(total) + (edge,)):
        side = jnp.where(lane == 2 + at, part, side)
    return side.astype(jnp.bfloat16)


def merge(states, valid, dv):
    between = jnp.zeros((1, 1), jnp.float32)
    heights, links = [], []
    for state, there in zip(states, valid):
        side = state[:16, dv:].astype(jnp.float32)[:1]
        peak = side[:, 2:3] + side[:, 3:4] + side[:, 4:5]
        total = side[:, 5:6] + side[:, 6:7] + side[:, 7:8]
        edge = side[:, 8:9]
        wanted = wanted if links else edge
        link = jnp.logical_and(edge == wanted, edge >= 0.0)
        if there is not None:
            link = jnp.logical_and(link, there)
        heights.append(jnp.where(link, peak + between, FAR_LOW))
        links.append(link)
        between = between + total
    top = heights[0]
    for height in heights[1:]:
        top = jnp.maximum(top, height)
    carry = None
    for state, height, link in zip(states, heights, links):
        part = jnp.where(link, jnp.exp(height - top), 0.0) * state[...].astype(jnp.float32)
        carry = part if carry is None else carry + part
    return carry, top, between, jnp.where(links[0], wanted, -1.0)


def put_state(out, carry, top, total, edge, dv):
    out[:, :dv] = carry[:, :dv].astype(jnp.bfloat16)
    sums = carry[:, dv : dv + 1] + carry[:, dv + 1 : dv + 2]
    out[:, dv:] = pack_side(sums, top, total, edge, (carry.shape[0], EXTRA))


def summary_kernel(info, keys, values, gates, give, mine):
    dqk = keys.shape[1]
    dv = values.shape[1]
    length = keys.shape[0]
    rows = gates[...]
    left, right = running_sums(log_sigmoid(rows))
    doc = rows[4:5]
    first, last = doc[:, :1], doc[:, length - 1 :]
    keys_t = keys[...].astype(jnp.float32).T
    vals = values[...]
    upper = info[0] == 1
    for cum, total, in_gate, edge, holder in (
        (left[2:3], left[2:3, length - 1 :], rows[0:1], last, upper),
        (right[3:4], right[3:4, :1], rows[1:2], first, jnp.logical_not(upper)),
    ):
        exponent = jnp.where(doc == edge, total - cum + in_gate, FAR_LOW)
        peak = jnp.max(exponent, axis=1, keepdims=True)
        weighted = (keys_t * jnp.exp(exponent - peak)).astype(jnp.bfloat16)
        memory = jnp.dot(weighted, vals, preferred_element_type=jnp.float32).astype(jnp.bfloat16)
        sums = jnp.sum(weighted.astype(jnp.float32), axis=1, keepdims=True)
        side = pack_side(sums, peak, total, edge, (dqk, EXTRA))

        @pl.when(holder)
        def _():
            mine[:, :dv] = memory
            mine[:, dv:] = side

        @pl.when(jnp.logical_not(holder))
        def _():
            give[:, :dv] = memory
            give[:, dv:] = side


SMALL = pl.BlockSpec(memory_space=pltpu.SMEM)
LOCAL = pl.BlockSpec(memory_space=pltpu.VMEM)


def summaries(info, keys, values, gates):
    shape = jax.ShapeDtypeStruct((keys.shape[1], values.shape[1] + EXTRA), jnp.bfloat16)
    return pl.pallas_call(
        summary_kernel,
        out_shape=(shape, shape),
        in_specs=[SMALL, LOCAL, LOCAL, LOCAL],
        name="summary",
    )(info, keys, values, gates)


def pair_kernel(mine, got, out):
    dv = mine.shape[1] - EXTRA
    put_state(out, *merge((mine, got), (None, None), dv), dv)


def pair_state(mine, got):
    return pl.pallas_call(
        pair_kernel, out_shape=jax.ShapeDtypeStruct(mine.shape, mine.dtype), name="pair"
    )(mine, got)


def lead_kernel(info, *refs):
    states, out = refs[:-1], refs[-1]
    dv = out.shape[1] - EXTRA
    valid = [info[1] > j for j in range(len(states))]
    put_state(out, *merge(states, valid, dv), dv)


def lead_state(info, states):
    return pl.pallas_call(
        lead_kernel,
        out_shape=jax.ShapeDtypeStruct(states[0].shape, states[0].dtype),
        in_specs=[SMALL] + [LOCAL] * len(states),
        name="lead",
    )(info, *states)


def intra_kernel(queries, keys, values, gates, num_f, num_b, stats, row_buf, col_buf):
    tile = queries.shape[0]
    step = pl.program_id(0)
    scale = queries.shape[1] ** (-0.5)

    @pl.when(step == 0)
    def _():
        rows = gates[...]
        left, right = running_sums(log_sigmoid(rows))
        doc = rows[4:5]
        cums = [left[2:3], right[3:4], rows[0:1] - left[2:3], rows[1:2] - right[3:4]]
        pack = jnp.concatenate(cums + [doc] * 4, axis=0)
        row_buf[...] = pack
        col_buf[...] = pack.T

    scores = (
        lax.dot_general(
            queries[...], keys[...], (((1,), (1,)), ((), ())), preferred_element_type=jnp.float32
        )
        * scale
    )
    cols = col_buf[pl.ds(step * tile, tile), :]
    rows = row_buf[...]
    at_t = step * tile + lax.broadcasted_iota(jnp.int32, scores.shape, 0)
    at_s = lax.broadcasted_iota(jnp.int32, scores.shape, 1)
    same = cols[:, 4:5] == rows[4:5]
    found = []
    for way, out in enumerate((num_f, num_b)):
        order = at_t >= at_s if way == 0 else at_t <= at_s
        keep = jnp.logical_and(order, same)
        inside = rows[2 + way : 3 + way]
        peak = jnp.max(jnp.where(keep, inside, FAR_LOW), axis=1, keepdims=True)
        weights = jnp.where(keep, scores * jnp.exp(inside - peak), 0.0)
        out[...] = jnp.dot(
            weights.astype(jnp.bfloat16), values[...], preferred_element_type=jnp.float32
        )
        found.append((cols[:, way : way + 1], peak, jnp.sum(weights, axis=1, keepdims=True)))
    lane = lax.broadcasted_iota(jnp.int32, (tile, LANES), 1)
    side = jnp.where(lane == 6, cols[:, 4:5], 0.0)
    for at, part in enumerate(found[0] + found[1]):
        side = jnp.where(lane == at, part, side)
    stats[...] = side


def intra(queries, keys, values, gates):
    length, dqk = queries.shape
    dv = values.shape[1]
    tile = length // 3 if length % 384 == 0 else length
    whole = lambda a: pl.BlockSpec(a.shape, lambda i: (0, 0))
    by_rows = lambda width: pl.BlockSpec((tile, width), lambda i: (i, 0))
    wide = lambda width: jax.ShapeDtypeStruct((length, width), jnp.float32)
    return pl.pallas_call(
        intra_kernel,
        out_shape=(wide(dv), wide(dv), wide(LANES)),
        grid=(length // tile,),
        in_specs=[by_rows(dqk), whole(keys), whole(values), whole(gates)],
        out_specs=(by_rows(dv), by_rows(dv), by_rows(LANES)),
        scratch_shapes=[pltpu.VMEM((8, length), jnp.float32), pltpu.VMEM((length, 8), jnp.float32)],
        name="intra",
    )(queries, keys, values, gates)


def emit_kernel(reach, info, queries, num_f, num_b, stats, out_gate, gain, *rest):
    states, handed = rest[: reach + 1], rest[reach + 1]
    outs, (carry_buf, top_buf) = rest[reach + 2 : -2], rest[-2:]
    dv = num_f.shape[1]
    step = pl.program_id(0)
    scale = queries.shape[1] ** (-0.5)

    @pl.when(step == 0)
    def _():
        valid = [None] + [info[1] > j for j in range(reach)]
        for way, got, there in ((1 - info[0], states, valid), (info[0], (handed,), (None,))):
            carry, top, _, edge = merge(got, there, dv)
            carry_buf[way, :, :dv] = carry[:, :dv].astype(jnp.bfloat16)
            sums = carry[:, dv : dv + 1] + carry[:, dv + 1 : dv + 2]
            carry_buf[way, :, dv:] = pack_side(sums, top, top, edge, (carry.shape[0], EXTRA))
            top_buf[way] = jnp.broadcast_to(jnp.concatenate([top, edge], axis=0), (2, LANES))

    query = queries[...]
    side = stats[...]
    memory = None
    for way, num in enumerate((num_f, num_b)):
        _, peak, denom = (side[:, 3 * way + k : 3 * way + k + 1] for k in range(3))
        usable = side[:, 6:7] == top_buf[way, 1:2, :1]
        carried = jnp.where(usable, top_buf[way, :1, :1], FAR_LOW)
        most = jnp.maximum(carried, peak)
        local = jnp.exp(peak - most)
        inter = jnp.where(usable, jnp.exp(carried - most), 0.0) * scale
        got = jnp.dot(query, carry_buf[way], preferred_element_type=jnp.float32)
        denom = denom * local + inter * (got[:, dv : dv + 1] + got[:, dv + 1 : dv + 2])
        share = 1.0 / jnp.maximum(jnp.abs(denom), 1.0)
        part = num[...] * (local * share) + got[:, :dv] * (inter * share)
        memory = part if memory is None else memory + part
    factor = lax.rsqrt(jnp.mean(memory * memory, axis=1, keepdims=True) + EPS)
    gate = 1.0 / (1.0 + jnp.exp(-out_gate[...].astype(jnp.float32)))
    readout = (memory * factor * gain[...] * gate).astype(jnp.bfloat16)
    for slot, out in enumerate(outs):

        @pl.when(info[2 + step] == slot)
        def _():
            out[...] = readout


def emit(info, queries, inner, out_gate, gain, states, handed, count):
    length, dqk = queries.shape
    num_f, num_b, stats = inner
    dv = num_f.shape[1]
    tile = length // count
    whole = lambda a: pl.BlockSpec(a.shape, lambda i, *_: (0, 0))
    by_rows = lambda width: pl.BlockSpec((tile, width), lambda i, *_: (i, 0))
    shape = jax.ShapeDtypeStruct((tile, dv), jnp.bfloat16)
    return pl.pallas_call(
        functools.partial(emit_kernel, len(states) - 1),
        out_shape=(shape,) * count,
        grid_spec=pltpu.PrefetchScalarGridSpec(
            num_scalar_prefetch=1,
            grid=(count,),
            in_specs=[by_rows(dqk), by_rows(dv), by_rows(dv), by_rows(LANES), by_rows(dv), whole(gain)]
            + [whole(s) for s in (*states, handed)],
            out_specs=(whole(shape),) * count,
            scratch_shapes=[
                pltpu.VMEM((2, dqk, dv + EXTRA), jnp.bfloat16),
                pltpu.VMEM((2, 2, LANES), jnp.float32),
            ],
        ),
        name="emit",
    )(info, queries, num_f, num_b, stats, out_gate, gain, *states, handed)


def project_kernel(count, turn, info, *refs):
    pieces, weights = refs[:count], refs[count : 2 * count]
    resid, gain, mixed_out, normed_out, beside_out, whole = refs[2 * count :]
    mixed = resid[...].astype(jnp.float32)
    for piece, weight in zip(pieces, weights):
        mixed = mixed + jnp.dot(piece[...], weight[...], preferred_element_type=jnp.float32)
    mixed_out[...] = mixed
    factor = lax.rsqrt(jnp.mean(mixed * mixed, axis=1, keepdims=True) + EPS)
    normed = mixed * factor * gain[...]
    if not turn:
        normed_out[...] = normed.astype(jnp.bfloat16)
        beside_out[...] = normed_out[...]
        return
    whole[...] = normed
    depth = mixed.shape[1] // turn
    for k in range(turn):
        at = pl.multiple_of(info[k] * depth, LANES)
        part = whole[:, pl.ds(at, depth)].astype(jnp.bfloat16)
        normed_out[:, k * depth : (k + 1) * depth] = part
        beside_out[:, (k ^ 1) * depth : ((k ^ 1) + 1) * depth] = part


def project(pieces, weights, resid, gain, sources, depth):
    inside = depth % LANES == 0
    mixed, normed, beside = pl.pallas_call(
        functools.partial(project_kernel, len(pieces), len(sources) if inside else 0),
        out_shape=(
            jax.ShapeDtypeStruct(resid.shape, jnp.float32),
            jax.ShapeDtypeStruct(resid.shape, jnp.bfloat16),
            jax.ShapeDtypeStruct(resid.shape, jnp.bfloat16),
        ),
        in_specs=[SMALL] + [LOCAL] * (2 * len(pieces) + 2),
        scratch_shapes=[pltpu.VMEM(resid.shape, jnp.float32)],
        name="project",
    )(jnp.stack(sources).astype(jnp.int32), *pieces, *weights, resid, gain)
    if not inside:
        cuts = [lax.dynamic_slice_in_dim(normed, at * depth, depth, 1) for at in sources]
        normed = jnp.concatenate(cuts, axis=1)
        beside = jnp.concatenate([cuts[k ^ 1] for k in range(len(cuts))], axis=1)
    return mixed, normed, beside


ANYWHERE = pl.BlockSpec(memory_space=pl.ANY)


def pack_kernel(*refs):
    parts, out, sems = refs[:-2], refs[-2], refs[-1]
    copies = [
        pltpu.make_async_copy(part, out.at[k], sems.at[k]) for k, part in enumerate(parts)
    ]
    for copy in copies:
        copy.start()
    for copy in copies:
        copy.wait()


def pack(parts):
    return pl.pallas_call(
        pack_kernel,
        out_shape=jax.ShapeDtypeStruct((len(parts),) + parts[0].shape, parts[0].dtype),
        in_specs=[ANYWHERE] * len(parts),
        out_specs=ANYWHERE,
        scratch_shapes=[pltpu.SemaphoreType.DMA((len(parts),))],
    )(*parts)


def up_kernel(blocks, steps, *refs):
    rows = refs[:blocks]
    mine = refs[blocks : blocks + steps]
    theirs = refs[blocks + steps : blocks + 2 * steps]
    out, row_buf, buf, sems = refs[blocks + 2 * steps :]
    each, depth, width = mine[0].shape
    copies, at = [], 0
    for k, source in enumerate(rows):
        span = pl.ds(at, source.shape[0])
        copies.append(pltpu.make_async_copy(source, row_buf.at[span], sems.at[k]))
        at += source.shape[0]
    for core, weights in enumerate((mine, theirs)):
        for k, weight in enumerate(weights):
            copies.append(
                pltpu.make_async_copy(
                    weight,
                    buf.at[core, pl.ds(k * each, each)],
                    sems.at[blocks + core * steps + k],
                )
            )
    for copy in copies:
        copy.start()
    for core in range(2):
        for copy in copies[: blocks + steps] if core == 0 else copies[blocks + steps :]:
            copy.wait()
        here = jnp.dot(
            row_buf[...],
            buf[core].reshape(steps * each * depth, width),
            preferred_element_type=jnp.float32,
        )
        out[:, core * width : (core + 1) * width] = jnp.square(jnp.maximum(here, 0.0)).astype(
            jnp.bfloat16
        )


def up_product(rows, mine, theirs):
    steps = len(mine)
    each, depth, width = mine[0].shape
    total = sum(r.shape[0] for r in rows)
    return pl.pallas_call(
        functools.partial(up_kernel, len(rows), steps),
        out_shape=jax.ShapeDtypeStruct((total, 2 * width), jnp.bfloat16),
        in_specs=[ANYWHERE] * (len(rows) + 2 * steps),
        scratch_shapes=[
            pltpu.VMEM((total, rows[0].shape[1]), jnp.bfloat16),
            pltpu.VMEM((2, steps * each, depth, width), jnp.bfloat16),
            pltpu.SemaphoreType.DMA((len(rows) + 2 * steps,)),
        ],
    )(*rows, *mine, *theirs)


def split_of(line_first):
    return ((0, 2), (1, 3)) if line_first else ((0, 1), (2, 3))


def down_kernel(orders, early, late, *refs):
    groups = len(orders)
    weights = refs[: 2 * groups]
    outs = refs[2 * groups : 4 * groups]
    buf, sems = refs[4 * groups :]
    split = early.shape[0]
    copies = [
        pltpu.make_async_copy(early, buf.at[pl.ds(0, split)], sems.at[0]),
        pltpu.make_async_copy(late, buf.at[pl.ds(split, late.shape[0])], sems.at[1]),
    ]
    for copy in copies:
        copy.start()
    for copy in copies:
        copy.wait()
    half = buf.shape[1] // 2
    rows = buf.shape[0] // 4
    for g, line_first in enumerate(orders):
        mine, theirs = weights[2 * g : 2 * g + 2]
        keep, send = outs[2 * g : 2 * g + 2]
        width = mine.shape[2]
        kept, sent = split_of(line_first)
        for k in range(2):
            part = jnp.dot(
                buf[:, :half], mine[k], preferred_element_type=jnp.float32
            ) + jnp.dot(buf[:, half:], theirs[k], preferred_element_type=jnp.float32)
            for at, block in enumerate(kept):
                keep[at * rows : (at + 1) * rows, k * width : (k + 1) * width] = part[
                    block * rows : (block + 1) * rows
                ]
            to = (1 - k) if line_first else k
            for at, block in enumerate(sent):
                send[at * rows : (at + 1) * rows, to * width : (to + 1) * width] = part[
                    block * rows : (block + 1) * rows
                ].astype(jnp.bfloat16)


def down_product(early, late, weights, orders):
    half = (early.shape[0] + late.shape[0]) // 2
    width = 2 * weights[0][0].shape[2]
    shapes = [
        jax.ShapeDtypeStruct((half, width), kind)
        for _ in orders
        for kind in (jnp.float32, jnp.bfloat16)
    ]
    flat = [w for pair in weights for w in pair]
    return pl.pallas_call(
        functools.partial(down_kernel, orders),
        out_shape=shapes,
        in_specs=[ANYWHERE] * 2 + [LOCAL] * len(flat),
        scratch_shapes=[
            pltpu.VMEM((2 * half, early.shape[1]), jnp.bfloat16),
            pltpu.SemaphoreType.DMA((2,)),
        ],
    )(early, late, *flat)


def add_kernel(kept, sent, turn, ours, theirs, keep, send):
    rows = keep.shape[0] // len(kept)
    add = lambda k: (
        ours[k * rows : (k + 1) * rows].astype(jnp.float32)
        + theirs[k * rows : (k + 1) * rows].astype(jnp.float32)
    )
    for at, k in enumerate(kept):
        keep[at * rows : (at + 1) * rows] = add(k)
    half = send.shape[1] // 2
    for at, k in enumerate(sent):
        value = add(k).astype(jnp.bfloat16)
        span = slice(at * rows, (at + 1) * rows)
        if turn:
            send[span, :half] = value[:, half:]
            send[span, half:] = value[:, :half]
        else:
            send[span] = value


def add_blocks(ours, theirs, kept, sent, turn):
    rows = ours.shape[0] // (len(kept) + len(sent))
    width = ours.shape[1]
    return pl.pallas_call(
        functools.partial(add_kernel, kept, sent, turn),
        out_shape=(
            jax.ShapeDtypeStruct((rows * len(kept), width), jnp.float32),
            jax.ShapeDtypeStruct((rows * len(sent), width), jnp.bfloat16),
        ),
    )(ours, theirs)


def finish_kernel(count, info, mixed, *refs):
    kept, got, out = refs[:count], refs[count : 2 * count], refs[-1]
    width = kept[0].shape[1] // 2
    for k in range(2 * count):
        at = pl.multiple_of(info[k] * width, LANES)
        cols = slice((k % 2) * width, (k % 2 + 1) * width)
        total = mixed[:, pl.ds(at, width)] + kept[k // 2][:, cols]
        total = total + got[k // 2][:, cols].astype(jnp.float32)
        out[:, pl.ds(at, width)] = total.astype(jnp.bfloat16)


def finish(sources, mixed, kept, got):
    width = kept[0].shape[1] // 2
    if width % LANES == 0:
        return pl.pallas_call(
            functools.partial(finish_kernel, len(kept)),
            out_shape=jax.ShapeDtypeStruct(mixed.shape, jnp.bfloat16),
            in_specs=[SMALL] + [LOCAL] * (1 + 2 * len(kept)),
            name="finish",
        )(jnp.stack(sources).astype(jnp.int32), mixed, *kept, *got)
    out = jnp.zeros(mixed.shape, jnp.bfloat16)
    for k, source in enumerate(sources):
        cols = slice((k % 2) * width, (k % 2 + 1) * width)
        total = lax.dynamic_slice_in_dim(mixed, source * width, width, 1) + kept[k // 2][:, cols]
        total = total + got[k // 2][:, cols].astype(jnp.float32)
        out = lax.dynamic_update_slice_in_dim(out, total.astype(jnp.bfloat16), source * width, 1)
    return out


def tp_slots():
    outer, a, c = places("tp")
    return [2 * ((d // 2 - a) % outer) + ((d % 2) ^ c) for d in range(2 * outer)]


def tp_exchange(blocks):
    got = [blocks[0]]
    for slot, block in enumerate(blocks[1:], 1):
        step, cross = slot // 2, slot % 2
        got.append(shift(block, "tp", step, cross))
    return got


def tp_weights(value):
    outer = places("tp")[0]
    got = []
    for step in range(outer):
        here = shift(value, "tp", step) if step else value
        got += [here, flip(here, "tp")]
    return got


def row_blocks(value, given):
    outer = places("tp")[0]
    assert outer == 2
    across = shift(value, "tp", 1)
    beside = neighbour(given)
    return (value, beside, across), shift(beside, "tp", 1)


def sum_back(keep, send, line_first):
    across = lambda x: shift(x, "tp", 1)
    along = lambda x: neighbour(x)
    hops = (along, across) if line_first else (across, along)
    keep, send = add_blocks(keep, hops[0](send), (0,), (1,), not line_first)
    return keep, hops[1](send)


def half_shards(shard, dim):
    outer, a, _ = places("sp")
    size = shard.shape[dim] // 2
    kept = lax.dynamic_slice_in_dim(shard, (a % 2) * size, size, dim)
    given = lax.dynamic_slice_in_dim(shard, (1 - a % 2) * size, size, dim)
    steps = [[kept, neighbour(given)]]
    for _ in range(1, outer // 2):
        steps.append([shift(x, "sp", 2) for x in steps[-1]])
    return steps


def both_cores(packed):
    return packed, flip(packed, "tp")


def up_shards(shard):
    mine, theirs = [], []
    for here in half_shards(shard, 1):
        there = [flip(x, "sp") for x in here]
        packed = pack(here + there)
        mine.append(packed)
        theirs.append(flip(packed, "tp"))
    return mine, theirs


def down_shards(shard):
    got = []
    for step, here in enumerate(half_shards(shard, 0)):
        packed = pack(here)
        if step == 0:
            there = flip(packed, "sp")
        else:
            there = [flip(x, "sp") for x in here]
            there = pack(there)
        got.append(both_cores(packed))
        got.append(both_cores(there))
    return got


def ring_sources():
    outer, a, c = places("sp")
    assert outer % 2 == 0
    return [
        2 * (((a - 2 * step) % outer) ^ k) + (c ^ cross)
        for step in range(outer // 2)
        for cross in range(2)
        for k in range(2)
    ]


def shards(
    queries,
    keys,
    values,
    out_gate,
    input_gates,
    forget_gates,
    doc_ids,
    head_gain,
    w_out,
    resid,
    norm_gain,
    w_up,
    w_down,
):
    length = queries.shape[0]
    heads = input_gates.shape[1]
    outer, a, c = places("sp")
    up_mine, up_theirs = up_shards(w_up)
    down_groups = down_shards(w_down)
    out_shards = tp_weights(w_out)

    reach = min(2 * outer - 1, -(-(LONGEST_DOC - 1) // length))
    hops = min(outer - 1, -(-reach // 2))
    doc_pos = doc_ids.astype(jnp.float32)[None]
    slots = tp_slots()
    info = jnp.stack([c, jnp.where(c == 1, a, outer - 1 - a)] + slots).astype(jnp.int32)
    readouts = []
    for h in range(heads):
        cut = lambda x: x.reshape(length, heads, -1)[:, h]
        k, v = cut(keys), cut(values)
        gates = jnp.concatenate(
            [input_gates[:, h], forget_gates[:, h], doc_pos, jnp.zeros((3, length), jnp.float32)]
        )
        give, mine = summaries(info, k, v, gates)
        got = flip(give, "sp")
        pair = pair_state(mine, got)
        ahead = [carry_shift(pair, j) for j in range(1, hops + 1)]
        handed = flip(lead_state(info, ahead), "sp")
        inner = intra(cut(queries), k, v, gates)
        gain = head_gain.reshape(heads, 1, -1)[h]
        readouts.append(
            emit(
                info, cut(queries), inner, cut(out_gate), gain, [got] + ahead, handed, len(slots)
            )
        )
    blocks = readouts[0]
    if heads > 1:
        blocks = [jnp.concatenate(b, axis=1) for b in zip(*readouts)]
    sources = ring_sources()
    mixed, normed, given = project(
        tp_exchange(blocks), out_shards, resid, norm_gain[None], sources, w_up.shape[0]
    )
    early, late = row_blocks(normed, given)
    early = up_product(early, up_mine, up_theirs)
    late = up_product([late], up_mine, up_theirs)

    parts = down_product(early, late, down_groups[:2], (False, True))
    for step in range(2, len(down_groups)):
        parts += down_product(early, late, down_groups[step : step + 1], (step % 2 == 1,))
    kept, got = [], []
    for step in range(len(down_groups)):
        keep, send = parts[2 * step : 2 * step + 2]
        keep, last = sum_back(keep, send, step % 2 == 1)
        kept.append(keep)
        got.append(last)
    return finish(sources, mixed, kept, got)


def solution(mesh):
    in_specs = (
        P("sp", "tp"),
        P("sp", "tp"),
        P("sp", "tp"),
        P("sp", "tp"),
        P(None, "tp", "sp"),
        P(None, "tp", "sp"),
        P("sp"),
        P("tp"),
        P("tp", None),
        P(("sp", "tp"), None),
        P(),
        P("sp", "tp"),
        P("tp", "sp"),
    )
    out_specs = P(("sp", "tp"), None)

    return jax.shard_map(shards, mesh=mesh, in_specs=in_specs, out_specs=out_specs, check_vma=False)
```

```python
import functools

import jax
import jax.numpy as jnp
from jax import lax
from jax.experimental import pallas as pl
from jax.experimental.pallas import tpu as pltpu
from jax.sharding import PartitionSpec as P

EPS = 1e-06
FAR_LOW = -1e30
LONGEST_DOC = 3072
LANES = 128
EXTRA = LANES


def places(axis):
    outer = lax.axis_size(axis) // 2
    assert outer * 2 == lax.axis_size(axis)
    index = lax.axis_index(axis)
    return outer, index // 2, index % 2


def flip(value, axis):
    return lax.ppermute(value, axis, [(i, i ^ 1) for i in range(lax.axis_size(axis))])


def shift(value, axis, step, cross=0):
    outer = lax.axis_size(axis) // 2
    moves = [
        (2 * a + c, 2 * ((a + step) % outer) + (c ^ cross)) for a in range(outer) for c in range(2)
    ]
    return lax.ppermute(value, axis, moves)


def neighbour(value):
    moves = [(i, i ^ 2) for i in range(lax.axis_size("sp"))]
    return lax.ppermute(value, "sp", moves)


def carry_shift(value, step):
    outer = lax.axis_size("sp") // 2
    moves = [(2 * a, 2 * (a - step)) for a in range(step, outer)]
    moves += [(2 * a + 1, 2 * (a + step) + 1) for a in range(outer - step)]
    return lax.ppermute(value, "sp", moves)


def running_sums(rows):
    length = rows.shape[1]
    lane = lax.broadcasted_iota(jnp.int32, rows.shape, 1)
    left, right = rows, rows
    step = 1
    while step < length:
        left = left + jnp.where(lane >= step, pltpu.roll(left, step, 1), 0.0)
        right = right + jnp.where(lane < length - step, pltpu.roll(right, length - step, 1), 0.0)
        step *= 2
    return left, right


def log_sigmoid(x):
    return jnp.minimum(x, 0.0) - jnp.log1p(jnp.exp(-jnp.abs(x)))


def three_parts(x):
    high = x.astype(jnp.bfloat16).astype(jnp.float32)
    rest = x - high
    mid = rest.astype(jnp.bfloat16).astype(jnp.float32)
    return high, mid, rest - mid


def pack_side(sums, peak, total, edge, shape):
    lane = lax.broadcasted_iota(jnp.int32, shape, 1)
    high = sums.astype(jnp.bfloat16).astype(jnp.float32)
    side = jnp.where(lane == 0, high, jnp.where(lane == 1, sums - high, 0.0))
    for at, part in enumerate(three_parts(peak) + three_parts(total) + (edge,)):
        side = jnp.where(lane == 2 + at, part, side)
    return side.astype(jnp.bfloat16)


def merge(states, valid, dv):
    between = jnp.zeros((1, 1), jnp.float32)
    heights, links = [], []
    for state, there in zip(states, valid):
        side = state[:16, dv:].astype(jnp.float32)[:1]
        peak = side[:, 2:3] + side[:, 3:4] + side[:, 4:5]
        total = side[:, 5:6] + side[:, 6:7] + side[:, 7:8]
        edge = side[:, 8:9]
        wanted = wanted if links else edge
        link = jnp.logical_and(edge == wanted, edge >= 0.0)
        if there is not None:
            link = jnp.logical_and(link, there)
        heights.append(jnp.where(link, peak + between, FAR_LOW))
        links.append(link)
        between = between + total
    top = heights[0]
    for height in heights[1:]:
        top = jnp.maximum(top, height)
    carry = None
    for state, height, link in zip(states, heights, links):
        part = jnp.where(link, jnp.exp(height - top), 0.0) * state[...].astype(jnp.float32)
        carry = part if carry is None else carry + part
    return carry, top, between, jnp.where(links[0], wanted, -1.0)


def put_state(out, carry, top, total, edge, dv):
    out[:, :dv] = carry[:, :dv].astype(jnp.bfloat16)
    sums = carry[:, dv : dv + 1] + carry[:, dv + 1 : dv + 2]
    out[:, dv:] = pack_side(sums, top, total, edge, (carry.shape[0], EXTRA))


def summary_kernel(info, keys, values, gates, give, mine):
    dqk = keys.shape[1]
    dv = values.shape[1]
    length = keys.shape[0]
    rows = gates[...]
    left, right = running_sums(log_sigmoid(rows))
    doc = rows[4:5]
    first, last = doc[:, :1], doc[:, length - 1 :]
    keys_t = keys[...].astype(jnp.float32).T
    vals = values[...]
    upper = info[0] == 1
    for cum, total, in_gate, edge, holder in (
        (left[2:3], left[2:3, length - 1 :], rows[0:1], last, upper),
        (right[3:4], right[3:4, :1], rows[1:2], first, jnp.logical_not(upper)),
    ):
        exponent = jnp.where(doc == edge, total - cum + in_gate, FAR_LOW)
        peak = jnp.max(exponent, axis=1, keepdims=True)
        weighted = (keys_t * jnp.exp(exponent - peak)).astype(jnp.bfloat16)
        memory = jnp.dot(weighted, vals, preferred_element_type=jnp.float32).astype(jnp.bfloat16)
        sums = jnp.sum(weighted.astype(jnp.float32), axis=1, keepdims=True)
        side = pack_side(sums, peak, total, edge, (dqk, EXTRA))

        @pl.when(holder)
        def _():
            mine[:, :dv] = memory
            mine[:, dv:] = side

        @pl.when(jnp.logical_not(holder))
        def _():
            give[:, :dv] = memory
            give[:, dv:] = side


def room(mib):
    return pltpu.CompilerParams(vmem_limit_bytes=mib << 20)


SMALL = pl.BlockSpec(memory_space=pltpu.SMEM)
LOCAL = pl.BlockSpec(memory_space=pltpu.VMEM)


def summaries(info, keys, values, gates):
    shape = jax.ShapeDtypeStruct((keys.shape[1], values.shape[1] + EXTRA), jnp.bfloat16)
    return pl.pallas_call(
        summary_kernel,
        out_shape=(shape, shape),
        in_specs=[SMALL, LOCAL, LOCAL, LOCAL],
        name="summary", compiler_params=room(10),
    )(info, keys, values, gates)


def pair_kernel(mine, got, out):
    dv = mine.shape[1] - EXTRA
    put_state(out, *merge((mine, got), (None, None), dv), dv)


def pair_state(mine, got):
    return pl.pallas_call(
        pair_kernel, out_shape=jax.ShapeDtypeStruct(mine.shape, mine.dtype), name="pair", compiler_params=room(5)
    )(mine, got)


def lead_kernel(info, *refs):
    states, out = refs[:-1], refs[-1]
    dv = out.shape[1] - EXTRA
    valid = [info[1] > j for j in range(len(states))]
    put_state(out, *merge(states, valid, dv), dv)


def lead_state(info, states):
    return pl.pallas_call(
        lead_kernel,
        out_shape=jax.ShapeDtypeStruct(states[0].shape, states[0].dtype),
        in_specs=[SMALL] + [LOCAL] * len(states),
        name="lead", compiler_params=room(5),
    )(info, *states)


def intra_kernel(queries, keys, values, gates, num_f, num_b, stats, row_buf, col_buf):
    tile = queries.shape[0]
    step = pl.program_id(0)
    scale = queries.shape[1] ** (-0.5)

    @pl.when(step == 0)
    def _():
        rows = gates[...]
        left, right = running_sums(log_sigmoid(rows))
        doc = rows[4:5]
        cums = [left[2:3], right[3:4], rows[0:1] - left[2:3], rows[1:2] - right[3:4]]
        pack = jnp.concatenate(cums + [doc] * 4, axis=0)
        row_buf[...] = pack
        col_buf[...] = pack.T

    scores = (
        lax.dot_general(
            queries[...], keys[...], (((1,), (1,)), ((), ())), preferred_element_type=jnp.float32
        )
        * scale
    )
    cols = col_buf[pl.ds(step * tile, tile), :]
    rows = row_buf[...]
    at_t = step * tile + lax.broadcasted_iota(jnp.int32, scores.shape, 0)
    at_s = lax.broadcasted_iota(jnp.int32, scores.shape, 1)
    same = cols[:, 4:5] == rows[4:5]
    found = []
    for way, out in enumerate((num_f, num_b)):
        order = at_t >= at_s if way == 0 else at_t <= at_s
        keep = jnp.logical_and(order, same)
        inside = rows[2 + way : 3 + way]
        peak = jnp.max(jnp.where(keep, inside, FAR_LOW), axis=1, keepdims=True)
        weights = jnp.where(keep, scores * jnp.exp(inside - peak), 0.0)
        out[...] = jnp.dot(
            weights.astype(jnp.bfloat16), values[...], preferred_element_type=jnp.float32
        )
        found.append((cols[:, way : way + 1], peak, jnp.sum(weights, axis=1, keepdims=True)))
    lane = lax.broadcasted_iota(jnp.int32, (tile, LANES), 1)
    side = jnp.where(lane == 6, cols[:, 4:5], 0.0)
    for at, part in enumerate(found[0] + found[1]):
        side = jnp.where(lane == at, part, side)
    stats[...] = side


def intra(queries, keys, values, gates):
    length, dqk = queries.shape
    dv = values.shape[1]
    tile = length // 3 if length % 384 == 0 else length
    whole = lambda a: pl.BlockSpec(a.shape, lambda i: (0, 0))
    by_rows = lambda width: pl.BlockSpec((tile, width), lambda i: (i, 0))
    wide = lambda width: jax.ShapeDtypeStruct((length, width), jnp.float32)
    return pl.pallas_call(
        intra_kernel,
        out_shape=(wide(dv), wide(dv), wide(LANES)),
        grid=(length // tile,),
        in_specs=[by_rows(dqk), whole(keys), whole(values), whole(gates)],
        out_specs=(by_rows(dv), by_rows(dv), by_rows(LANES)),
        scratch_shapes=[pltpu.VMEM((8, length), jnp.float32), pltpu.VMEM((length, 8), jnp.float32)],
        name="intra", compiler_params=room(16),
    )(queries, keys, values, gates)


def emit_kernel(reach, info, queries, num_f, num_b, stats, out_gate, gain, *rest):
    states, handed = rest[: reach + 1], rest[reach + 1]
    outs, (carry_buf, top_buf) = rest[reach + 2 : -2], rest[-2:]
    dv = num_f.shape[1]
    step = pl.program_id(0)
    scale = queries.shape[1] ** (-0.5)

    @pl.when(step == 0)
    def _():
        valid = [None] + [info[1] > j for j in range(reach)]
        for way, got, there in ((1 - info[0], states, valid), (info[0], (handed,), (None,))):
            carry, top, _, edge = merge(got, there, dv)
            carry_buf[way, :, :dv] = carry[:, :dv].astype(jnp.bfloat16)
            sums = carry[:, dv : dv + 1] + carry[:, dv + 1 : dv + 2]
            carry_buf[way, :, dv:] = pack_side(sums, top, top, edge, (carry.shape[0], EXTRA))
            top_buf[way] = jnp.broadcast_to(jnp.concatenate([top, edge], axis=0), (2, LANES))

    query = queries[...]
    side = stats[...]
    memory = None
    for way, num in enumerate((num_f, num_b)):
        _, peak, denom = (side[:, 3 * way + k : 3 * way + k + 1] for k in range(3))
        usable = side[:, 6:7] == top_buf[way, 1:2, :1]
        carried = jnp.where(usable, top_buf[way, :1, :1], FAR_LOW)
        most = jnp.maximum(carried, peak)
        local = jnp.exp(peak - most)
        inter = jnp.where(usable, jnp.exp(carried - most), 0.0) * scale
        got = jnp.dot(query, carry_buf[way], preferred_element_type=jnp.float32)
        denom = denom * local + inter * (got[:, dv : dv + 1] + got[:, dv + 1 : dv + 2])
        share = 1.0 / jnp.maximum(jnp.abs(denom), 1.0)
        part = num[...] * (local * share) + got[:, :dv] * (inter * share)
        memory = part if memory is None else memory + part
    factor = lax.rsqrt(jnp.mean(memory * memory, axis=1, keepdims=True) + EPS)
    gate = 1.0 / (1.0 + jnp.exp(-out_gate[...].astype(jnp.float32)))
    readout = (memory * factor * gain[...] * gate).astype(jnp.bfloat16)
    for slot, out in enumerate(outs):

        @pl.when(info[2 + step] == slot)
        def _():
            out[...] = readout


def emit(info, queries, inner, out_gate, gain, states, handed, count):
    length, dqk = queries.shape
    num_f, num_b, stats = inner
    dv = num_f.shape[1]
    tile = length // count
    whole = lambda a: pl.BlockSpec(a.shape, lambda i, *_: (0, 0))
    by_rows = lambda width: pl.BlockSpec((tile, width), lambda i, *_: (i, 0))
    shape = jax.ShapeDtypeStruct((tile, dv), jnp.bfloat16)
    return pl.pallas_call(
        functools.partial(emit_kernel, len(states) - 1),
        out_shape=(shape,) * count,
        grid_spec=pltpu.PrefetchScalarGridSpec(
            num_scalar_prefetch=1,
            grid=(count,),
            in_specs=[by_rows(dqk), by_rows(dv), by_rows(dv), by_rows(LANES), by_rows(dv), whole(gain)]
            + [whole(s) for s in (*states, handed)],
            out_specs=(whole(shape),) * count,
            scratch_shapes=[
                pltpu.VMEM((2, dqk, dv + EXTRA), jnp.bfloat16),
                pltpu.VMEM((2, 2, LANES), jnp.float32),
            ],
        ),
        name="emit", compiler_params=room(12),
    )(info, queries, num_f, num_b, stats, out_gate, gain, *states, handed)


def project_kernel(count, turn, info, *refs):
    pieces, weights = refs[:count], refs[count : 2 * count]
    resid, gain, mixed_out, normed_out, beside_out, whole = refs[2 * count :]
    mixed = resid[...].astype(jnp.float32)
    for piece, weight in zip(pieces, weights):
        mixed = mixed + jnp.dot(piece[...], weight[...], preferred_element_type=jnp.float32)
    mixed_out[...] = mixed
    factor = lax.rsqrt(jnp.mean(mixed * mixed, axis=1, keepdims=True) + EPS)
    normed = mixed * factor * gain[...]
    if not turn:
        normed_out[...] = normed.astype(jnp.bfloat16)
        beside_out[...] = normed_out[...]
        return
    whole[...] = normed
    depth = mixed.shape[1] // turn
    for k in range(turn):
        at = pl.multiple_of(info[k] * depth, LANES)
        part = whole[:, pl.ds(at, depth)].astype(jnp.bfloat16)
        normed_out[:, k * depth : (k + 1) * depth] = part
        beside_out[:, (k ^ 1) * depth : ((k ^ 1) + 1) * depth] = part


def project(pieces, weights, resid, gain, sources, depth):
    inside = depth % LANES == 0
    mixed, normed, beside = pl.pallas_call(
        functools.partial(project_kernel, len(pieces), len(sources) if inside else 0),
        out_shape=(
            jax.ShapeDtypeStruct(resid.shape, jnp.float32),
            jax.ShapeDtypeStruct(resid.shape, jnp.bfloat16),
            jax.ShapeDtypeStruct(resid.shape, jnp.bfloat16),
        ),
        in_specs=[SMALL] + [LOCAL] * (2 * len(pieces) + 2),
        scratch_shapes=[pltpu.VMEM(resid.shape, jnp.float32)],
        name="project", compiler_params=room(20),
    )(jnp.stack(sources).astype(jnp.int32), *pieces, *weights, resid, gain)
    if not inside:
        cuts = [lax.dynamic_slice_in_dim(normed, at * depth, depth, 1) for at in sources]
        normed = jnp.concatenate(cuts, axis=1)
        beside = jnp.concatenate([cuts[k ^ 1] for k in range(len(cuts))], axis=1)
    return mixed, normed, beside


def pack_kernel(*refs):
    for k, part in enumerate(refs[:-1]):
        refs[-1][k] = part[...]


def pack(parts):
    return pl.pallas_call(
        pack_kernel,
        out_shape=jax.ShapeDtypeStruct((len(parts),) + parts[0].shape, parts[0].dtype),
        compiler_params=room(8),
    )(*parts)


def up_kernel(blocks, steps, *refs):
    rows = refs[:blocks]
    mine = refs[blocks : blocks + steps]
    theirs = refs[blocks + steps : blocks + 2 * steps]
    out, row_buf = refs[blocks + 2 * steps :]
    each, depth, width = mine[0].shape
    at = 0
    for source in rows:
        row_buf[at : at + source.shape[0]] = source[...]
        at += source.shape[0]
    span = each * depth
    for core, weights in enumerate((mine, theirs)):
        here = None
        for k, weight in enumerate(weights):
            part = jnp.dot(
                row_buf[:, k * span : (k + 1) * span],
                weight[...].reshape(span, width),
                preferred_element_type=jnp.float32,
            )
            here = part if here is None else here + part
        out[:, core * width : (core + 1) * width] = jnp.square(jnp.maximum(here, 0.0)).astype(
            jnp.bfloat16
        )


def up_product(rows, mine, theirs):
    steps = len(mine)
    width = mine[0].shape[2]
    total = sum(r.shape[0] for r in rows)
    return pl.pallas_call(
        functools.partial(up_kernel, len(rows), steps),
        out_shape=jax.ShapeDtypeStruct((total, 2 * width), jnp.bfloat16),
        scratch_shapes=[pltpu.VMEM((total, rows[0].shape[1]), jnp.bfloat16)],
        compiler_params=room(26),
    )(*rows, *mine, *theirs)


def split_of(line_first):
    return ((0, 2), (1, 3)) if line_first else ((0, 1), (2, 3))


def down_kernel(orders, early, late, *refs):
    groups = len(orders)
    weights = refs[: 2 * groups]
    outs = refs[2 * groups : 4 * groups]
    wide = refs[4 * groups]
    half = early.shape[1] // 2
    rows = (early.shape[0] + late.shape[0]) // 4
    width = weights[0].shape[2]
    for g, line_first in enumerate(orders):
        for core in range(2):
            for k in range(2):
                wide[core * half : (core + 1) * half, k * width : (k + 1) * width] = weights[
                    2 * g + core
                ][k]
        keep, send = outs[2 * g : 2 * g + 2]
        kept, sent = split_of(line_first)
        first = 0
        for hidden in (early, late):
            part = jnp.dot(hidden[...], wide[...], preferred_element_type=jnp.float32)
            for k in range(hidden.shape[0] // rows):
                value = part[k * rows : (k + 1) * rows]
                block = first + k
                if block in kept:
                    at = kept.index(block) * rows
                    keep[at : at + rows] = value
                    continue
                at = sent.index(block) * rows
                value = value.astype(jnp.bfloat16)
                if line_first:
                    send[at : at + rows, :width] = value[:, width:]
                    send[at : at + rows, width:] = value[:, :width]
                else:
                    send[at : at + rows] = value
            first += hidden.shape[0] // rows


def down_product(early, late, weights, orders):
    half = (early.shape[0] + late.shape[0]) // 2
    width = 2 * weights[0][0].shape[2]
    shapes = [
        jax.ShapeDtypeStruct((half, width), kind)
        for _ in orders
        for kind in (jnp.float32, jnp.bfloat16)
    ]
    flat = [w for pair in weights for w in pair]
    return pl.pallas_call(
        functools.partial(down_kernel, orders),
        out_shape=shapes,
        scratch_shapes=[pltpu.VMEM((early.shape[1], width), jnp.bfloat16)],
        compiler_params=room(18),
    )(early, late, *flat)


def add_kernel(kept, sent, turn, ours, theirs, keep, send):
    rows = keep.shape[0] // len(kept)
    add = lambda k: (
        ours[k * rows : (k + 1) * rows].astype(jnp.float32)
        + theirs[k * rows : (k + 1) * rows].astype(jnp.float32)
    )
    for at, k in enumerate(kept):
        keep[at * rows : (at + 1) * rows] = add(k)
    half = send.shape[1] // 2
    for at, k in enumerate(sent):
        value = add(k).astype(jnp.bfloat16)
        span = slice(at * rows, (at + 1) * rows)
        if turn:
            send[span, :half] = value[:, half:]
            send[span, half:] = value[:, :half]
        else:
            send[span] = value


def add_blocks(ours, theirs, kept, sent, turn):
    rows = ours.shape[0] // (len(kept) + len(sent))
    width = ours.shape[1]
    return pl.pallas_call(
        functools.partial(add_kernel, kept, sent, turn),
        out_shape=(
            jax.ShapeDtypeStruct((rows * len(kept), width), jnp.float32),
            jax.ShapeDtypeStruct((rows * len(sent), width), jnp.bfloat16),
        ),
        compiler_params=room(5),
    )(ours, theirs)


def finish_kernel(count, info, mixed, *refs):
    kept, got, out = refs[:count], refs[count : 2 * count], refs[-1]
    width = kept[0].shape[1] // 2
    for k in range(2 * count):
        at = pl.multiple_of(info[k] * width, LANES)
        cols = slice((k % 2) * width, (k % 2 + 1) * width)
        total = mixed[:, pl.ds(at, width)] + kept[k // 2][:, cols]
        total = total + got[k // 2][:, cols].astype(jnp.float32)
        out[:, pl.ds(at, width)] = total.astype(jnp.bfloat16)


def finish(sources, mixed, kept, got):
    width = kept[0].shape[1] // 2
    if width % LANES == 0:
        return pl.pallas_call(
            functools.partial(finish_kernel, len(kept)),
            out_shape=jax.ShapeDtypeStruct(mixed.shape, jnp.bfloat16),
            in_specs=[SMALL] + [LOCAL] * (1 + 2 * len(kept)),
            name="finish", compiler_params=room(8),
        )(jnp.stack(sources).astype(jnp.int32), mixed, *kept, *got)
    out = jnp.zeros(mixed.shape, jnp.bfloat16)
    for k, source in enumerate(sources):
        cols = slice((k % 2) * width, (k % 2 + 1) * width)
        total = lax.dynamic_slice_in_dim(mixed, source * width, width, 1) + kept[k // 2][:, cols]
        total = total + got[k // 2][:, cols].astype(jnp.float32)
        out = lax.dynamic_update_slice_in_dim(out, total.astype(jnp.bfloat16), source * width, 1)
    return out


def tp_slots():
    outer, a, c = places("tp")
    return [2 * ((d // 2 - a) % outer) + ((d % 2) ^ c) for d in range(2 * outer)]


def tp_exchange(blocks):
    got = [blocks[0]]
    for slot, block in enumerate(blocks[1:], 1):
        step, cross = slot // 2, slot % 2
        got.append(shift(block, "tp", step, cross))
    return got


def tp_weights(value):
    outer = places("tp")[0]
    got = []
    for step in range(outer):
        here = shift(value, "tp", step) if step else value
        got += [here, flip(here, "tp")]
    return got


def row_blocks(value, given):
    outer = places("tp")[0]
    assert outer == 2
    across = shift(value, "tp", 1)
    beside = neighbour(given)
    return (value, beside, across), shift(beside, "tp", 1)


def sum_back(keep, send, line_first):
    across = lambda x: shift(x, "tp", 1)
    along = lambda x: neighbour(x)
    hops = (along, across) if line_first else (across, along)
    keep, send = add_blocks(keep, hops[0](send), (0,), (1,), not line_first)
    return keep, hops[1](send)


def half_shards(shard, dim):
    outer, a, _ = places("sp")
    size = shard.shape[dim] // 2
    kept = lax.dynamic_slice_in_dim(shard, (a % 2) * size, size, dim)
    given = lax.dynamic_slice_in_dim(shard, (1 - a % 2) * size, size, dim)
    steps = [[kept, neighbour(given)]]
    for _ in range(1, outer // 2):
        steps.append([shift(x, "sp", 2) for x in steps[-1]])
    return steps


def both_cores(packed):
    return packed, flip(packed, "tp")


def up_shards(shard):
    mine, theirs = [], []
    for here in half_shards(shard, 1):
        there = [flip(x, "sp") for x in here]
        packed = pack(here + there)
        mine.append(packed)
        theirs.append(flip(packed, "tp"))
    return mine, theirs


def down_shards(shard):
    got = []
    for step, here in enumerate(half_shards(shard, 0)):
        packed = pack(here)
        if step == 0:
            there = flip(packed, "sp")
        else:
            there = [flip(x, "sp") for x in here]
            there = pack(there)
        got.append(both_cores(packed))
        got.append(both_cores(there))
    return got


def ring_sources():
    outer, a, c = places("sp")
    assert outer % 2 == 0
    return [
        2 * (((a - 2 * step) % outer) ^ k) + (c ^ cross)
        for step in range(outer // 2)
        for cross in range(2)
        for k in range(2)
    ]


def shards(
    queries,
    keys,
    values,
    out_gate,
    input_gates,
    forget_gates,
    doc_ids,
    head_gain,
    w_out,
    resid,
    norm_gain,
    w_up,
    w_down,
):
    length = queries.shape[0]
    heads = input_gates.shape[1]
    outer, a, c = places("sp")
    up_mine, up_theirs = up_shards(w_up)
    down_groups = down_shards(w_down)
    out_shards = tp_weights(w_out)

    reach = min(2 * outer - 1, -(-(LONGEST_DOC - 1) // length))
    hops = min(outer - 1, -(-reach // 2))
    doc_pos = doc_ids.astype(jnp.float32)[None]
    slots = tp_slots()
    info = jnp.stack([c, jnp.where(c == 1, a, outer - 1 - a)] + slots).astype(jnp.int32)
    readouts = []
    for h in range(heads):
        cut = lambda x: x.reshape(length, heads, -1)[:, h]
        k, v = cut(keys), cut(values)
        gates = jnp.concatenate(
            [input_gates[:, h], forget_gates[:, h], doc_pos, jnp.zeros((3, length), jnp.float32)]
        )
        give, mine = summaries(info, k, v, gates)
        got = flip(give, "sp")
        pair = pair_state(mine, got)
        ahead = [carry_shift(pair, j) for j in range(1, hops + 1)]
        handed = flip(lead_state(info, ahead), "sp")
        inner = intra(cut(queries), k, v, gates)
        gain = head_gain.reshape(heads, 1, -1)[h]
        readouts.append(
            emit(
                info, cut(queries), inner, cut(out_gate), gain, [got] + ahead, handed, len(slots)
            )
        )
    blocks = readouts[0]
    if heads > 1:
        blocks = [jnp.concatenate(b, axis=1) for b in zip(*readouts)]
    sources = ring_sources()
    mixed, normed, given = project(
        tp_exchange(blocks), out_shards, resid, norm_gain[None], sources, w_up.shape[0]
    )
    early, late = row_blocks(normed, given)
    early = up_product(early, up_mine, up_theirs)
    late = up_product([late], up_mine, up_theirs)

    parts = down_product(early, late, down_groups[:2], (False, True))
    for step in range(2, len(down_groups)):
        parts += down_product(early, late, down_groups[step : step + 1], (step % 2 == 1,))
    kept, got = [], []
    for step in range(len(down_groups)):
        keep, send = parts[2 * step : 2 * step + 2]
        keep, last = sum_back(keep, send, step % 2 == 1)
        kept.append(keep)
        got.append(last)
    return finish(sources, mixed, kept, got)


def solution(mesh):
    in_specs = (
        P("sp", "tp"),
        P("sp", "tp"),
        P("sp", "tp"),
        P("sp", "tp"),
        P(None, "tp", "sp"),
        P(None, "tp", "sp"),
        P("sp"),
        P("tp"),
        P("tp", None),
        P(("sp", "tp"), None),
        P(),
        P("sp", "tp"),
        P("tp", "sp"),
    )
    out_specs = P(("sp", "tp"), None)

    return jax.shard_map(shards, mesh=mesh, in_specs=in_specs, out_specs=out_specs, check_vma=False)
```

```python
import functools

import jax
import jax.numpy as jnp
from jax import lax
from jax.experimental import pallas as pl
from jax.experimental.pallas import tpu as pltpu
from jax.sharding import PartitionSpec as P

EPS = 1e-06
FAR_LOW = -1e30
LONGEST_DOC = 3072
LANES = 128
EXTRA = LANES


def places(axis):
    outer = lax.axis_size(axis) // 2
    assert outer * 2 == lax.axis_size(axis)
    index = lax.axis_index(axis)
    return outer, index // 2, index % 2


def flip(value, axis):
    return lax.ppermute(value, axis, [(i, i ^ 1) for i in range(lax.axis_size(axis))])


def shift(value, axis, step, cross=0):
    outer = lax.axis_size(axis) // 2
    moves = [
        (2 * a + c, 2 * ((a + step) % outer) + (c ^ cross)) for a in range(outer) for c in range(2)
    ]
    return lax.ppermute(value, axis, moves)


def neighbour(value):
    moves = [(i, i ^ 2) for i in range(lax.axis_size("sp"))]
    return lax.ppermute(value, "sp", moves)


def skew(value):
    outer = lax.axis_size("sp") // 2
    moves = [(2 * a + c, 2 * (((a + 2) % outer) ^ 1) + c) for a in range(outer) for c in range(2)]
    return lax.ppermute(value, "sp", moves)


def carry_shift(value, step):
    outer = lax.axis_size("sp") // 2
    moves = [(2 * a, 2 * (a - step)) for a in range(step, outer)]
    moves += [(2 * a + 1, 2 * (a + step) + 1) for a in range(outer - step)]
    return lax.ppermute(value, "sp", moves)


def running_sums(rows):
    length = rows.shape[1]
    lane = lax.broadcasted_iota(jnp.int32, rows.shape, 1)
    left, right = rows, rows
    step = 1
    while step < length:
        left = left + jnp.where(lane >= step, pltpu.roll(left, step, 1), 0.0)
        right = right + jnp.where(lane < length - step, pltpu.roll(right, length - step, 1), 0.0)
        step *= 2
    return left, right


def log_sigmoid(x):
    return jnp.minimum(x, 0.0) - jnp.log1p(jnp.exp(-jnp.abs(x)))


def three_parts(x):
    high = x.astype(jnp.bfloat16).astype(jnp.float32)
    rest = x - high
    mid = rest.astype(jnp.bfloat16).astype(jnp.float32)
    return high, mid, rest - mid


def pack_side(sums, peak, total, edge, shape):
    lane = lax.broadcasted_iota(jnp.int32, shape, 1)
    high = sums.astype(jnp.bfloat16).astype(jnp.float32)
    side = jnp.where(lane == 0, high, jnp.where(lane == 1, sums - high, 0.0))
    for at, part in enumerate(three_parts(peak) + three_parts(total) + (edge,)):
        side = jnp.where(lane == 2 + at, part, side)
    return side.astype(jnp.bfloat16)


def merge(states, valid, dv):
    between = jnp.zeros((1, 1), jnp.float32)
    heights, links = [], []
    for state, there in zip(states, valid):
        side = state[:16, dv:].astype(jnp.float32)[:1]
        peak = side[:, 2:3] + side[:, 3:4] + side[:, 4:5]
        total = side[:, 5:6] + side[:, 6:7] + side[:, 7:8]
        edge = side[:, 8:9]
        wanted = wanted if links else edge
        link = jnp.logical_and(edge == wanted, edge >= 0.0)
        if there is not None:
            link = jnp.logical_and(link, there)
        heights.append(jnp.where(link, peak + between, FAR_LOW))
        links.append(link)
        between = between + total
    top = heights[0]
    for height in heights[1:]:
        top = jnp.maximum(top, height)
    carry = None
    for state, height, link in zip(states, heights, links):
        part = jnp.where(link, jnp.exp(height - top), 0.0) * state[...].astype(jnp.float32)
        carry = part if carry is None else carry + part
    return carry, top, between, jnp.where(links[0], wanted, -1.0)


def put_state(out, carry, top, total, edge, dv):
    out[:, :dv] = carry[:, :dv].astype(jnp.bfloat16)
    sums = carry[:, dv : dv + 1] + carry[:, dv + 1 : dv + 2]
    out[:, dv:] = pack_side(sums, top, total, edge, (carry.shape[0], EXTRA))


def summary_kernel(info, keys, values, gates, give, mine):
    dqk = keys.shape[1]
    dv = values.shape[1]
    length = keys.shape[0]
    rows = gates[...]
    left, right = running_sums(log_sigmoid(rows))
    doc = rows[4:5]
    first, last = doc[:, :1], doc[:, length - 1 :]
    keys_t = keys[...].astype(jnp.float32).T
    vals = values[...]
    upper = info[0] == 1
    for cum, total, in_gate, edge, holder in (
        (left[2:3], left[2:3, length - 1 :], rows[0:1], last, upper),
        (right[3:4], right[3:4, :1], rows[1:2], first, jnp.logical_not(upper)),
    ):
        exponent = jnp.where(doc == edge, total - cum + in_gate, FAR_LOW)
        peak = jnp.max(exponent, axis=1, keepdims=True)
        weighted = (keys_t * jnp.exp(exponent - peak)).astype(jnp.bfloat16)
        memory = jnp.dot(weighted, vals, preferred_element_type=jnp.float32).astype(jnp.bfloat16)
        sums = jnp.sum(weighted.astype(jnp.float32), axis=1, keepdims=True)
        side = pack_side(sums, peak, total, edge, (dqk, EXTRA))

        @pl.when(holder)
        def _():
            mine[:, :dv] = memory
            mine[:, dv:] = side

        @pl.when(jnp.logical_not(holder))
        def _():
            give[:, :dv] = memory
            give[:, dv:] = side


def room(mib):
    return pltpu.CompilerParams(vmem_limit_bytes=mib << 20)


SMALL = pl.BlockSpec(memory_space=pltpu.SMEM)
LOCAL = pl.BlockSpec(memory_space=pltpu.VMEM)


def summaries(info, keys, values, gates):
    shape = jax.ShapeDtypeStruct((keys.shape[1], values.shape[1] + EXTRA), jnp.bfloat16)
    return pl.pallas_call(
        summary_kernel,
        out_shape=(shape, shape),
        in_specs=[SMALL, LOCAL, LOCAL, LOCAL],
        name="summary", compiler_params=room(10),
    )(info, keys, values, gates)


def pair_kernel(mine, got, out):
    dv = mine.shape[1] - EXTRA
    put_state(out, *merge((mine, got), (None, None), dv), dv)


def pair_state(mine, got):
    return pl.pallas_call(
        pair_kernel, out_shape=jax.ShapeDtypeStruct(mine.shape, mine.dtype), name="pair", compiler_params=room(5)
    )(mine, got)


def lead_kernel(info, *refs):
    states, out = refs[:-1], refs[-1]
    dv = out.shape[1] - EXTRA
    valid = [info[1] > j for j in range(len(states))]
    put_state(out, *merge(states, valid, dv), dv)


def lead_state(info, states):
    return pl.pallas_call(
        lead_kernel,
        out_shape=jax.ShapeDtypeStruct(states[0].shape, states[0].dtype),
        in_specs=[SMALL] + [LOCAL] * len(states),
        name="lead", compiler_params=room(5),
    )(info, *states)


def intra_kernel(queries, keys, values, gates, num_f, num_b, stats, row_buf, col_buf):
    tile = queries.shape[0]
    step = pl.program_id(0)
    scale = queries.shape[1] ** (-0.5)

    @pl.when(step == 0)
    def _():
        rows = gates[...]
        left, right = running_sums(log_sigmoid(rows))
        doc = rows[4:5]
        cums = [left[2:3], right[3:4], rows[0:1] - left[2:3], rows[1:2] - right[3:4]]
        pack = jnp.concatenate(cums + [doc] * 4, axis=0)
        row_buf[...] = pack
        col_buf[...] = pack.T

    scores = (
        lax.dot_general(
            queries[...], keys[...], (((1,), (1,)), ((), ())), preferred_element_type=jnp.float32
        )
        * scale
    )
    cols = col_buf[pl.ds(step * tile, tile), :]
    rows = row_buf[...]
    at_t = step * tile + lax.broadcasted_iota(jnp.int32, scores.shape, 0)
    at_s = lax.broadcasted_iota(jnp.int32, scores.shape, 1)
    same = cols[:, 4:5] == rows[4:5]
    found = []
    for way, out in enumerate((num_f, num_b)):
        order = at_t >= at_s if way == 0 else at_t <= at_s
        keep = jnp.logical_and(order, same)
        inside = rows[2 + way : 3 + way]
        peak = jnp.max(jnp.where(keep, inside, FAR_LOW), axis=1, keepdims=True)
        weights = jnp.where(keep, scores * jnp.exp(inside - peak), 0.0)
        out[...] = jnp.dot(
            weights.astype(jnp.bfloat16), values[...], preferred_element_type=jnp.float32
        )
        found.append((cols[:, way : way + 1], peak, jnp.sum(weights, axis=1, keepdims=True)))
    lane = lax.broadcasted_iota(jnp.int32, (tile, LANES), 1)
    side = jnp.where(lane == 6, cols[:, 4:5], 0.0)
    for at, part in enumerate(found[0] + found[1]):
        side = jnp.where(lane == at, part, side)
    stats[...] = side


def intra(queries, keys, values, gates):
    length, dqk = queries.shape
    dv = values.shape[1]
    tile = length // 3 if length % 384 == 0 else length
    whole = lambda a: pl.BlockSpec(a.shape, lambda i: (0, 0))
    by_rows = lambda width: pl.BlockSpec((tile, width), lambda i: (i, 0))
    wide = lambda width: jax.ShapeDtypeStruct((length, width), jnp.float32)
    return pl.pallas_call(
        intra_kernel,
        out_shape=(wide(dv), wide(dv), wide(LANES)),
        grid=(length // tile,),
        in_specs=[by_rows(dqk), whole(keys), whole(values), whole(gates)],
        out_specs=(by_rows(dv), by_rows(dv), by_rows(LANES)),
        scratch_shapes=[pltpu.VMEM((8, length), jnp.float32), pltpu.VMEM((length, 8), jnp.float32)],
        name="intra", compiler_params=room(16),
    )(queries, keys, values, gates)


def emit_kernel(reach, info, queries, num_f, num_b, stats, out_gate, gain, *rest):
    states, handed = rest[: reach + 1], rest[reach + 1]
    outs, (carry_buf, top_buf) = rest[reach + 2 : -2], rest[-2:]
    dv = num_f.shape[1]
    step = pl.program_id(0)
    scale = queries.shape[1] ** (-0.5)

    @pl.when(step == 0)
    def _():
        valid = [None] + [info[1] > j for j in range(reach)]
        for way, got, there in ((1 - info[0], states, valid), (info[0], (handed,), (None,))):
            carry, top, _, edge = merge(got, there, dv)
            carry_buf[way, :, :dv] = carry[:, :dv].astype(jnp.bfloat16)
            sums = carry[:, dv : dv + 1] + carry[:, dv + 1 : dv + 2]
            carry_buf[way, :, dv:] = pack_side(sums, top, top, edge, (carry.shape[0], EXTRA))
            top_buf[way] = jnp.broadcast_to(jnp.concatenate([top, edge], axis=0), (2, LANES))

    query = queries[...]
    side = stats[...]
    memory = None
    for way, num in enumerate((num_f, num_b)):
        _, peak, denom = (side[:, 3 * way + k : 3 * way + k + 1] for k in range(3))
        usable = side[:, 6:7] == top_buf[way, 1:2, :1]
        carried = jnp.where(usable, top_buf[way, :1, :1], FAR_LOW)
        most = jnp.maximum(carried, peak)
        local = jnp.exp(peak - most)
        inter = jnp.where(usable, jnp.exp(carried - most), 0.0) * scale
        got = jnp.dot(query, carry_buf[way], preferred_element_type=jnp.float32)
        denom = denom * local + inter * (got[:, dv : dv + 1] + got[:, dv + 1 : dv + 2])
        share = 1.0 / jnp.maximum(jnp.abs(denom), 1.0)
        part = num[...] * (local * share) + got[:, :dv] * (inter * share)
        memory = part if memory is None else memory + part
    factor = lax.rsqrt(jnp.mean(memory * memory, axis=1, keepdims=True) + EPS)
    gate = 1.0 / (1.0 + jnp.exp(-out_gate[...].astype(jnp.float32)))
    readout = (memory * factor * gain[...] * gate).astype(jnp.bfloat16)
    for slot, out in enumerate(outs):

        @pl.when(info[2 + step] == slot)
        def _():
            out[...] = readout


def emit(info, queries, inner, out_gate, gain, states, handed, count):
    length, dqk = queries.shape
    num_f, num_b, stats = inner
    dv = num_f.shape[1]
    tile = length // count
    whole = lambda a: pl.BlockSpec(a.shape, lambda i, *_: (0, 0))
    by_rows = lambda width: pl.BlockSpec((tile, width), lambda i, *_: (i, 0))
    shape = jax.ShapeDtypeStruct((tile, dv), jnp.bfloat16)
    return pl.pallas_call(
        functools.partial(emit_kernel, len(states) - 1),
        out_shape=(shape,) * count,
        grid_spec=pltpu.PrefetchScalarGridSpec(
            num_scalar_prefetch=1,
            grid=(count,),
            in_specs=[by_rows(dqk), by_rows(dv), by_rows(dv), by_rows(LANES), by_rows(dv), whole(gain)]
            + [whole(s) for s in (*states, handed)],
            out_specs=(whole(shape),) * count,
            scratch_shapes=[
                pltpu.VMEM((2, dqk, dv + EXTRA), jnp.bfloat16),
                pltpu.VMEM((2, 2, LANES), jnp.float32),
            ],
        ),
        name="emit", compiler_params=room(12),
    )(info, queries, num_f, num_b, stats, out_gate, gain, *states, handed)


def project_kernel(count, turn, info, *refs):
    pieces, weights = refs[:count], refs[count : 2 * count]
    resid, gain, mixed_out, normed_out, beside_out, whole = refs[2 * count :]
    mixed = resid[...].astype(jnp.float32)
    for piece, weight in zip(pieces, weights):
        mixed = mixed + jnp.dot(piece[...], weight[...], preferred_element_type=jnp.float32)
    mixed_out[...] = mixed
    factor = lax.rsqrt(jnp.mean(mixed * mixed, axis=1, keepdims=True) + EPS)
    normed = mixed * factor * gain[...]
    if not turn:
        normed_out[...] = normed.astype(jnp.bfloat16)
        beside_out[...] = normed_out[...]
        return
    whole[...] = normed
    depth = mixed.shape[1] // turn
    for k in range(turn):
        at = pl.multiple_of(info[k] * depth, LANES)
        part = whole[:, pl.ds(at, depth)].astype(jnp.bfloat16)
        normed_out[:, k * depth : (k + 1) * depth] = part
        beside_out[:, (k ^ 1) * depth : ((k ^ 1) + 1) * depth] = part


def project(pieces, weights, resid, gain, sources, depth):
    inside = depth % LANES == 0
    mixed, normed, beside = pl.pallas_call(
        functools.partial(project_kernel, len(pieces), len(sources) if inside else 0),
        out_shape=(
            jax.ShapeDtypeStruct(resid.shape, jnp.float32),
            jax.ShapeDtypeStruct(resid.shape, jnp.bfloat16),
            jax.ShapeDtypeStruct(resid.shape, jnp.bfloat16),
        ),
        in_specs=[SMALL] + [LOCAL] * (2 * len(pieces) + 2),
        scratch_shapes=[pltpu.VMEM(resid.shape, jnp.float32)],
        name="project", compiler_params=room(20),
    )(jnp.stack(sources).astype(jnp.int32), *pieces, *weights, resid, gain)
    if not inside:
        cuts = [lax.dynamic_slice_in_dim(normed, at * depth, depth, 1) for at in sources]
        normed = jnp.concatenate(cuts, axis=1)
        beside = jnp.concatenate([cuts[k ^ 1] for k in range(len(cuts))], axis=1)
    return mixed, normed, beside


def pack_kernel(*refs):
    for k, part in enumerate(refs[:-1]):
        refs[-1][k] = part[...]


def pack(parts):
    return pl.pallas_call(
        pack_kernel,
        out_shape=jax.ShapeDtypeStruct((len(parts),) + parts[0].shape, parts[0].dtype),
        compiler_params=room(8),
    )(*parts)


def up_kernel(blocks, steps, *refs):
    rows = refs[:blocks]
    mine = refs[blocks : blocks + steps]
    theirs = refs[blocks + steps : blocks + 2 * steps]
    out, row_buf = refs[blocks + 2 * steps :]
    each, depth, width = mine[0].shape
    at = 0
    for source in rows:
        row_buf[at : at + source.shape[0]] = source[...]
        at += source.shape[0]
    span = each * depth
    for core, weights in enumerate((mine, theirs)):
        here = None
        for k, weight in enumerate(weights):
            part = jnp.dot(
                row_buf[:, k * span : (k + 1) * span],
                weight[...].reshape(span, width),
                preferred_element_type=jnp.float32,
            )
            here = part if here is None else here + part
        out[:, core * width : (core + 1) * width] = jnp.square(jnp.maximum(here, 0.0)).astype(
            jnp.bfloat16
        )


def up_product(rows, mine, theirs):
    steps = len(mine)
    width = mine[0].shape[2]
    total = sum(r.shape[0] for r in rows)
    return pl.pallas_call(
        functools.partial(up_kernel, len(rows), steps),
        out_shape=jax.ShapeDtypeStruct((total, 2 * width), jnp.bfloat16),
        scratch_shapes=[pltpu.VMEM((total, rows[0].shape[1]), jnp.bfloat16)],
        compiler_params=room(26),
    )(*rows, *mine, *theirs)


def split_of(line_first):
    return ((0, 2), (1, 3)) if line_first else ((0, 1), (2, 3))


def down_kernel(orders, early, late, *refs):
    groups = len(orders)
    weights = refs[: 2 * groups]
    outs = refs[2 * groups : 4 * groups]
    wide = refs[4 * groups]
    half = early.shape[1] // 2
    rows = (early.shape[0] + late.shape[0]) // 4
    width = weights[0].shape[2]
    for g, line_first in enumerate(orders):
        for core in range(2):
            for k in range(2):
                wide[core * half : (core + 1) * half, k * width : (k + 1) * width] = weights[
                    2 * g + core
                ][k]
        keep, send = outs[2 * g : 2 * g + 2]
        kept, sent = split_of(line_first)
        first = 0
        for hidden in (early, late):
            part = jnp.dot(hidden[...], wide[...], preferred_element_type=jnp.float32)
            for k in range(hidden.shape[0] // rows):
                value = part[k * rows : (k + 1) * rows]
                block = first + k
                if block in kept:
                    at = kept.index(block) * rows
                    keep[at : at + rows] = value
                    continue
                at = sent.index(block) * rows
                value = value.astype(jnp.bfloat16)
                if line_first:
                    send[at : at + rows, :width] = value[:, width:]
                    send[at : at + rows, width:] = value[:, :width]
                else:
                    send[at : at + rows] = value
            first += hidden.shape[0] // rows


def down_product(early, late, weights, orders):
    half = (early.shape[0] + late.shape[0]) // 2
    width = 2 * weights[0][0].shape[2]
    shapes = [
        jax.ShapeDtypeStruct((half, width), kind)
        for _ in orders
        for kind in (jnp.float32, jnp.bfloat16)
    ]
    flat = [w for pair in weights for w in pair]
    return pl.pallas_call(
        functools.partial(down_kernel, orders),
        out_shape=shapes,
        scratch_shapes=[pltpu.VMEM((early.shape[1], width), jnp.bfloat16)],
        compiler_params=room(18),
    )(early, late, *flat)


def add_kernel(kept, sent, turn, ours, theirs, keep, send):
    rows = keep.shape[0] // len(kept)
    add = lambda k: (
        ours[k * rows : (k + 1) * rows].astype(jnp.float32)
        + theirs[k * rows : (k + 1) * rows].astype(jnp.float32)
    )
    for at, k in enumerate(kept):
        keep[at * rows : (at + 1) * rows] = add(k)
    half = send.shape[1] // 2
    for at, k in enumerate(sent):
        value = add(k).astype(jnp.bfloat16)
        span = slice(at * rows, (at + 1) * rows)
        if turn:
            send[span, :half] = value[:, half:]
            send[span, half:] = value[:, :half]
        else:
            send[span] = value


def add_blocks(ours, theirs, kept, sent, turn):
    rows = ours.shape[0] // (len(kept) + len(sent))
    width = ours.shape[1]
    return pl.pallas_call(
        functools.partial(add_kernel, kept, sent, turn),
        out_shape=(
            jax.ShapeDtypeStruct((rows * len(kept), width), jnp.float32),
            jax.ShapeDtypeStruct((rows * len(sent), width), jnp.bfloat16),
        ),
        compiler_params=room(5),
    )(ours, theirs)


def finish_kernel(count, info, mixed, *refs):
    kept, got, out = refs[:count], refs[count : 2 * count], refs[-1]
    width = kept[0].shape[1] // 2
    for k in range(2 * count):
        at = pl.multiple_of(info[k] * width, LANES)
        cols = slice((k % 2) * width, (k % 2 + 1) * width)
        total = mixed[:, pl.ds(at, width)] + kept[k // 2][:, cols]
        total = total + got[k // 2][:, cols].astype(jnp.float32)
        out[:, pl.ds(at, width)] = total.astype(jnp.bfloat16)


def finish(sources, mixed, kept, got):
    width = kept[0].shape[1] // 2
    if width % LANES == 0:
        return pl.pallas_call(
            functools.partial(finish_kernel, len(kept)),
            out_shape=jax.ShapeDtypeStruct(mixed.shape, jnp.bfloat16),
            in_specs=[SMALL] + [LOCAL] * (1 + 2 * len(kept)),
            name="finish", compiler_params=room(8),
        )(jnp.stack(sources).astype(jnp.int32), mixed, *kept, *got)
    out = jnp.zeros(mixed.shape, jnp.bfloat16)
    for k, source in enumerate(sources):
        cols = slice((k % 2) * width, (k % 2 + 1) * width)
        total = lax.dynamic_slice_in_dim(mixed, source * width, width, 1) + kept[k // 2][:, cols]
        total = total + got[k // 2][:, cols].astype(jnp.float32)
        out = lax.dynamic_update_slice_in_dim(out, total.astype(jnp.bfloat16), source * width, 1)
    return out


def tp_slots():
    outer, a, c = places("tp")
    return [2 * ((d // 2 - a) % outer) + ((d % 2) ^ c) for d in range(2 * outer)]


def tp_exchange(blocks):
    got = [blocks[0]]
    for slot, block in enumerate(blocks[1:], 1):
        step, cross = slot // 2, slot % 2
        got.append(shift(block, "tp", step, cross))
    return got


def tp_weights(value):
    outer = places("tp")[0]
    got = []
    for step in range(outer):
        here = shift(value, "tp", step) if step else value
        got += [here, flip(here, "tp")]
    return got


def row_blocks(value, given):
    outer = places("tp")[0]
    assert outer == 2
    across = shift(value, "tp", 1)
    beside = neighbour(given)
    return (value, beside, across), shift(beside, "tp", 1)


def sum_back(keep, send, line_first):
    across = lambda x: shift(x, "tp", 1)
    along = lambda x: neighbour(x)
    hops = (along, across) if line_first else (across, along)
    keep, send = add_blocks(keep, hops[0](send), (0,), (1,), not line_first)
    return keep, hops[1](send)


def half_shards(shard, dim):
    outer, a, _ = places("sp")
    size = shard.shape[dim] // 2
    kept = lax.dynamic_slice_in_dim(shard, (a % 2) * size, size, dim)
    given = lax.dynamic_slice_in_dim(shard, (1 - a % 2) * size, size, dim)
    steps = [[kept, neighbour(given)]]
    for step in range(1, outer // 2):
        first = shift(steps[-1][0], "sp", 2)
        if step == 1:
            second = skew(given)
        else:
            second = shift(steps[-1][1], "sp", 2)
        steps.append([first, second])
    return steps


def both_cores(packed):
    return packed, flip(packed, "tp")


def up_shards(shard):
    mine, theirs = [], []
    for here in half_shards(shard, 1):
        there = [flip(x, "sp") for x in here]
        packed = pack(here + there)
        mine.append(packed)
        theirs.append(flip(packed, "tp"))
    return mine, theirs


def down_shards(shard):
    got = []
    for here in half_shards(shard, 0):
        packed = pack(here)
        there = [flip(x, "sp") for x in here]
        there = pack(there)
        got.append(both_cores(packed))
        got.append(both_cores(there))
    return got


def ring_sources():
    outer, a, c = places("sp")
    assert outer % 2 == 0
    return [
        2 * (((a - 2 * step) % outer) ^ k) + (c ^ cross)
        for step in range(outer // 2)
        for cross in range(2)
        for k in range(2)
    ]


def shards(
    queries,
    keys,
    values,
    out_gate,
    input_gates,
    forget_gates,
    doc_ids,
    head_gain,
    w_out,
    resid,
    norm_gain,
    w_up,
    w_down,
):
    length = queries.shape[0]
    heads = input_gates.shape[1]
    outer, a, c = places("sp")
    up_mine, up_theirs = up_shards(w_up)
    down_groups = down_shards(w_down)
    out_shards = tp_weights(w_out)

    reach = min(2 * outer - 1, -(-(LONGEST_DOC - 1) // length))
    hops = min(outer - 1, -(-reach // 2))
    doc_pos = doc_ids.astype(jnp.float32)[None]
    slots = tp_slots()
    info = jnp.stack([c, jnp.where(c == 1, a, outer - 1 - a)] + slots).astype(jnp.int32)
    readouts = []
    for h in range(heads):
        cut = lambda x: x.reshape(length, heads, -1)[:, h]
        k, v = cut(keys), cut(values)
        gates = jnp.concatenate(
            [input_gates[:, h], forget_gates[:, h], doc_pos, jnp.zeros((3, length), jnp.float32)]
        )
        give, mine = summaries(info, k, v, gates)
        got = flip(give, "sp")
        pair = pair_state(mine, got)
        ahead = [carry_shift(pair, j) for j in range(1, hops + 1)]
        handed = flip(lead_state(info, ahead), "sp")
        inner = intra(cut(queries), k, v, gates)
        gain = head_gain.reshape(heads, 1, -1)[h]
        readouts.append(
            emit(
                info, cut(queries), inner, cut(out_gate), gain, [got] + ahead, handed, len(slots)
            )
        )
    blocks = readouts[0]
    if heads > 1:
        blocks = [jnp.concatenate(b, axis=1) for b in zip(*readouts)]
    sources = ring_sources()
    mixed, normed, given = project(
        tp_exchange(blocks), out_shards, resid, norm_gain[None], sources, w_up.shape[0]
    )
    early, late = row_blocks(normed, given)
    early = up_product(early, up_mine, up_theirs)
    late = up_product([late], up_mine, up_theirs)

    parts = down_product(early, late, down_groups[:2], (False, True))
    for step in range(2, len(down_groups)):
        parts += down_product(early, late, down_groups[step : step + 1], (step % 2 == 1,))
    kept, got = [], []
    for step in range(len(down_groups)):
        keep, send = parts[2 * step : 2 * step + 2]
        keep, last = sum_back(keep, send, step % 2 == 1)
        kept.append(keep)
        got.append(last)
    return finish(sources, mixed, kept, got)


def solution(mesh):
    in_specs = (
        P("sp", "tp"),
        P("sp", "tp"),
        P("sp", "tp"),
        P("sp", "tp"),
        P(None, "tp", "sp"),
        P(None, "tp", "sp"),
        P("sp"),
        P("tp"),
        P("tp", None),
        P(("sp", "tp"), None),
        P(),
        P("sp", "tp"),
        P("tp", "sp"),
    )
    out_specs = P(("sp", "tp"), None)

    return jax.shard_map(shards, mesh=mesh, in_specs=in_specs, out_specs=out_specs, check_vma=False)
```

```python
import functools

import jax
import jax.numpy as jnp
from jax import lax
from jax.experimental import pallas as pl
from jax.experimental.pallas import tpu as pltpu
from jax.sharding import PartitionSpec as P

EPS = 1e-06
FAR_LOW = -1e30
LONGEST_DOC = 3072
LANES = 128
EXTRA = LANES


def places(axis):
    outer = lax.axis_size(axis) // 2
    assert outer * 2 == lax.axis_size(axis)
    index = lax.axis_index(axis)
    return outer, index // 2, index % 2


def flip(value, axis):
    return lax.ppermute(value, axis, [(i, i ^ 1) for i in range(lax.axis_size(axis))])


def shift(value, axis, step, cross=0):
    outer = lax.axis_size(axis) // 2
    moves = [
        (2 * a + c, 2 * ((a + step) % outer) + (c ^ cross)) for a in range(outer) for c in range(2)
    ]
    return lax.ppermute(value, axis, moves)


def neighbour(value):
    moves = [(i, i ^ 2) for i in range(lax.axis_size("sp"))]
    return lax.ppermute(value, "sp", moves)


def skew(value):
    outer = lax.axis_size("sp") // 2
    moves = [(2 * a + c, 2 * (((a + 2) % outer) ^ 1) + c) for a in range(outer) for c in range(2)]
    return lax.ppermute(value, "sp", moves)


def carry_shift(value, step):
    outer = lax.axis_size("sp") // 2
    moves = [(2 * a, 2 * (a - step)) for a in range(step, outer)]
    moves += [(2 * a + 1, 2 * (a + step) + 1) for a in range(outer - step)]
    return lax.ppermute(value, "sp", moves)


def running_sums(rows):
    length = rows.shape[1]
    lane = lax.broadcasted_iota(jnp.int32, rows.shape, 1)
    left, right = rows, rows
    step = 1
    while step < length:
        left = left + jnp.where(lane >= step, pltpu.roll(left, step, 1), 0.0)
        right = right + jnp.where(lane < length - step, pltpu.roll(right, length - step, 1), 0.0)
        step *= 2
    return left, right


def log_sigmoid(x):
    return jnp.minimum(x, 0.0) - jnp.log1p(jnp.exp(-jnp.abs(x)))


def three_parts(x):
    high = x.astype(jnp.bfloat16).astype(jnp.float32)
    rest = x - high
    mid = rest.astype(jnp.bfloat16).astype(jnp.float32)
    return high, mid, rest - mid


def pack_side(sums, peak, total, edge, shape):
    lane = lax.broadcasted_iota(jnp.int32, shape, 1)
    high = sums.astype(jnp.bfloat16).astype(jnp.float32)
    side = jnp.where(lane == 0, high, jnp.where(lane == 1, sums - high, 0.0))
    for at, part in enumerate(three_parts(peak) + three_parts(total) + (edge,)):
        side = jnp.where(lane == 2 + at, part, side)
    return side.astype(jnp.bfloat16)


def merge(states, valid, dv):
    between = jnp.zeros((1, 1), jnp.float32)
    heights, links = [], []
    for state, there in zip(states, valid):
        side = state[:16, dv:].astype(jnp.float32)[:1]
        peak = side[:, 2:3] + side[:, 3:4] + side[:, 4:5]
        total = side[:, 5:6] + side[:, 6:7] + side[:, 7:8]
        edge = side[:, 8:9]
        wanted = wanted if links else edge
        link = jnp.logical_and(edge == wanted, edge >= 0.0)
        if there is not None:
            link = jnp.logical_and(link, there)
        heights.append(jnp.where(link, peak + between, FAR_LOW))
        links.append(link)
        between = between + total
    top = heights[0]
    for height in heights[1:]:
        top = jnp.maximum(top, height)
    carry = None
    for state, height, link in zip(states, heights, links):
        part = jnp.where(link, jnp.exp(height - top), 0.0) * state[...].astype(jnp.float32)
        carry = part if carry is None else carry + part
    return carry, top, between, jnp.where(links[0], wanted, -1.0)


def put_state(out, carry, top, total, edge, dv):
    out[:, :dv] = carry[:, :dv].astype(jnp.bfloat16)
    sums = carry[:, dv : dv + 1] + carry[:, dv + 1 : dv + 2]
    out[:, dv:] = pack_side(sums, top, total, edge, (carry.shape[0], EXTRA))


def summary_kernel(info, keys, values, gates, give, mine):
    dqk = keys.shape[1]
    dv = values.shape[1]
    length = keys.shape[0]
    rows = gates[...]
    left, right = running_sums(log_sigmoid(rows))
    doc = rows[4:5]
    first, last = doc[:, :1], doc[:, length - 1 :]
    keys_t = keys[...].astype(jnp.float32).T
    vals = values[...]
    upper = info[0] == 1
    for cum, total, in_gate, edge, holder in (
        (left[2:3], left[2:3, length - 1 :], rows[0:1], last, upper),
        (right[3:4], right[3:4, :1], rows[1:2], first, jnp.logical_not(upper)),
    ):
        exponent = jnp.where(doc == edge, total - cum + in_gate, FAR_LOW)
        peak = jnp.max(exponent, axis=1, keepdims=True)
        weighted = (keys_t * jnp.exp(exponent - peak)).astype(jnp.bfloat16)
        memory = jnp.dot(weighted, vals, preferred_element_type=jnp.float32).astype(jnp.bfloat16)
        sums = jnp.sum(weighted.astype(jnp.float32), axis=1, keepdims=True)
        side = pack_side(sums, peak, total, edge, (dqk, EXTRA))

        @pl.when(holder)
        def _():
            mine[:, :dv] = memory
            mine[:, dv:] = side

        @pl.when(jnp.logical_not(holder))
        def _():
            give[:, :dv] = memory
            give[:, dv:] = side


def room(mib):
    return pltpu.CompilerParams(vmem_limit_bytes=mib << 20)


SMALL = pl.BlockSpec(memory_space=pltpu.SMEM)
LOCAL = pl.BlockSpec(memory_space=pltpu.VMEM)


def summaries(info, keys, values, gates):
    shape = jax.ShapeDtypeStruct((keys.shape[1], values.shape[1] + EXTRA), jnp.bfloat16)
    return pl.pallas_call(
        summary_kernel,
        out_shape=(shape, shape),
        in_specs=[SMALL, LOCAL, LOCAL, LOCAL],
        name="summary", compiler_params=room(10),
    )(info, keys, values, gates)


def pair_kernel(mine, got, out):
    dv = mine.shape[1] - EXTRA
    put_state(out, *merge((mine, got), (None, None), dv), dv)


def pair_state(mine, got):
    return pl.pallas_call(
        pair_kernel, out_shape=jax.ShapeDtypeStruct(mine.shape, mine.dtype), name="pair", compiler_params=room(5)
    )(mine, got)


def lead_kernel(info, *refs):
    states, out = refs[:-1], refs[-1]
    dv = out.shape[1] - EXTRA
    valid = [info[1] > j for j in range(len(states))]
    put_state(out, *merge(states, valid, dv), dv)


def lead_state(info, states):
    return pl.pallas_call(
        lead_kernel,
        out_shape=jax.ShapeDtypeStruct(states[0].shape, states[0].dtype),
        in_specs=[SMALL] + [LOCAL] * len(states),
        name="lead", compiler_params=room(5),
    )(info, *states)


def intra_kernel(queries, keys, values, gates, num_f, num_b, stats, row_buf, col_buf):
    tile = queries.shape[0]
    step = pl.program_id(0)
    scale = queries.shape[1] ** (-0.5)

    @pl.when(step == 0)
    def _():
        rows = gates[...]
        left, right = running_sums(log_sigmoid(rows))
        doc = rows[4:5]
        cums = [left[2:3], right[3:4], rows[0:1] - left[2:3], rows[1:2] - right[3:4]]
        pack = jnp.concatenate(cums + [doc] * 4, axis=0)
        row_buf[...] = pack
        col_buf[...] = pack.T

    scores = (
        lax.dot_general(
            queries[...], keys[...], (((1,), (1,)), ((), ())), preferred_element_type=jnp.float32
        )
        * scale
    )
    cols = col_buf[pl.ds(step * tile, tile), :]
    rows = row_buf[...]
    at_t = step * tile + lax.broadcasted_iota(jnp.int32, scores.shape, 0)
    at_s = lax.broadcasted_iota(jnp.int32, scores.shape, 1)
    same = cols[:, 4:5] == rows[4:5]
    found = []
    for way, out in enumerate((num_f, num_b)):
        order = at_t >= at_s if way == 0 else at_t <= at_s
        keep = jnp.logical_and(order, same)
        inside = rows[2 + way : 3 + way]
        peak = jnp.max(jnp.where(keep, inside, FAR_LOW), axis=1, keepdims=True)
        weights = jnp.where(keep, scores * jnp.exp(inside - peak), 0.0)
        out[...] = jnp.dot(
            weights.astype(jnp.bfloat16), values[...], preferred_element_type=jnp.float32
        )
        found.append((cols[:, way : way + 1], peak, jnp.sum(weights, axis=1, keepdims=True)))
    lane = lax.broadcasted_iota(jnp.int32, (tile, LANES), 1)
    side = jnp.where(lane == 6, cols[:, 4:5], 0.0)
    for at, part in enumerate(found[0] + found[1]):
        side = jnp.where(lane == at, part, side)
    stats[...] = side


def intra(queries, keys, values, gates):
    length, dqk = queries.shape
    dv = values.shape[1]
    tile = length // 3 if length % 384 == 0 else length
    whole = lambda a: pl.BlockSpec(a.shape, lambda i: (0, 0))
    by_rows = lambda width: pl.BlockSpec((tile, width), lambda i: (i, 0))
    wide = lambda width: jax.ShapeDtypeStruct((length, width), jnp.float32)
    return pl.pallas_call(
        intra_kernel,
        out_shape=(wide(dv), wide(dv), wide(LANES)),
        grid=(length // tile,),
        in_specs=[by_rows(dqk), whole(keys), whole(values), whole(gates)],
        out_specs=(by_rows(dv), by_rows(dv), by_rows(LANES)),
        scratch_shapes=[pltpu.VMEM((8, length), jnp.float32), pltpu.VMEM((length, 8), jnp.float32)],
        name="intra", compiler_params=room(16),
    )(queries, keys, values, gates)


def emit_kernel(reach, info, queries, num_f, num_b, stats, out_gate, gain, *rest):
    states, handed = rest[: reach + 1], rest[reach + 1]
    outs, (carry_buf, top_buf) = rest[reach + 2 : -2], rest[-2:]
    dv = num_f.shape[1]
    step = pl.program_id(0)
    scale = queries.shape[1] ** (-0.5)

    @pl.when(step == 0)
    def _():
        valid = [None] + [info[1] > j for j in range(reach)]
        for way, got, there in ((1 - info[0], states, valid), (info[0], (handed,), (None,))):
            carry, top, _, edge = merge(got, there, dv)
            carry_buf[way, :, :dv] = carry[:, :dv].astype(jnp.bfloat16)
            sums = carry[:, dv : dv + 1] + carry[:, dv + 1 : dv + 2]
            carry_buf[way, :, dv:] = pack_side(sums, top, top, edge, (carry.shape[0], EXTRA))
            top_buf[way] = jnp.broadcast_to(jnp.concatenate([top, edge], axis=0), (2, LANES))

    query = queries[...]
    side = stats[...]
    memory = None
    for way, num in enumerate((num_f, num_b)):
        _, peak, denom = (side[:, 3 * way + k : 3 * way + k + 1] for k in range(3))
        usable = side[:, 6:7] == top_buf[way, 1:2, :1]
        carried = jnp.where(usable, top_buf[way, :1, :1], FAR_LOW)
        most = jnp.maximum(carried, peak)
        local = jnp.exp(peak - most)
        inter = jnp.where(usable, jnp.exp(carried - most), 0.0) * scale
        got = jnp.dot(query, carry_buf[way], preferred_element_type=jnp.float32)
        denom = denom * local + inter * (got[:, dv : dv + 1] + got[:, dv + 1 : dv + 2])
        share = 1.0 / jnp.maximum(jnp.abs(denom), 1.0)
        part = num[...] * (local * share) + got[:, :dv] * (inter * share)
        memory = part if memory is None else memory + part
    factor = lax.rsqrt(jnp.mean(memory * memory, axis=1, keepdims=True) + EPS)
    gate = 1.0 / (1.0 + jnp.exp(-out_gate[...].astype(jnp.float32)))
    readout = (memory * factor * gain[...] * gate).astype(jnp.bfloat16)
    for slot, out in enumerate(outs):

        @pl.when(info[2 + step] == slot)
        def _():
            out[...] = readout


def emit(info, queries, inner, out_gate, gain, states, handed, count):
    length, dqk = queries.shape
    num_f, num_b, stats = inner
    dv = num_f.shape[1]
    tile = length // count
    whole = lambda a: pl.BlockSpec(a.shape, lambda i, *_: (0, 0))
    by_rows = lambda width: pl.BlockSpec((tile, width), lambda i, *_: (i, 0))
    shape = jax.ShapeDtypeStruct((tile, dv), jnp.bfloat16)
    return pl.pallas_call(
        functools.partial(emit_kernel, len(states) - 1),
        out_shape=(shape,) * count,
        grid_spec=pltpu.PrefetchScalarGridSpec(
            num_scalar_prefetch=1,
            grid=(count,),
            in_specs=[by_rows(dqk), by_rows(dv), by_rows(dv), by_rows(LANES), by_rows(dv), whole(gain)]
            + [whole(s) for s in (*states, handed)],
            out_specs=(whole(shape),) * count,
            scratch_shapes=[
                pltpu.VMEM((2, dqk, dv + EXTRA), jnp.bfloat16),
                pltpu.VMEM((2, 2, LANES), jnp.float32),
            ],
        ),
        name="emit", compiler_params=room(12),
    )(info, queries, num_f, num_b, stats, out_gate, gain, *states, handed)


def project_kernel(count, turn, info, *refs):
    pieces, weights = refs[:count], refs[count : 2 * count]
    resid, gain, mixed_out, normed_out, beside_top, beside_low, whole = refs[2 * count :]
    top = beside_top.shape[0]
    mixed = resid[...].astype(jnp.float32)
    for piece, weight in zip(pieces, weights):
        mixed = mixed + jnp.dot(piece[...], weight[...], preferred_element_type=jnp.float32)
    mixed_out[...] = mixed
    factor = lax.rsqrt(jnp.mean(mixed * mixed, axis=1, keepdims=True) + EPS)
    normed = mixed * factor * gain[...]
    if not turn:
        normed_out[...] = normed.astype(jnp.bfloat16)
        beside_top[...] = normed_out[:top]
        beside_low[...] = normed_out[top:]
        return
    whole[...] = normed
    depth = mixed.shape[1] // turn
    for k in range(turn):
        at = pl.multiple_of(info[k] * depth, LANES)
        part = whole[:, pl.ds(at, depth)].astype(jnp.bfloat16)
        normed_out[:, k * depth : (k + 1) * depth] = part
        beside_top[:, (k ^ 1) * depth : ((k ^ 1) + 1) * depth] = part[:top]
        beside_low[:, (k ^ 1) * depth : ((k ^ 1) + 1) * depth] = part[top:]


def project(pieces, weights, resid, gain, sources, depth):
    inside = depth % LANES == 0
    half = jax.ShapeDtypeStruct((resid.shape[0] // 2, resid.shape[1]), jnp.bfloat16)
    mixed, normed, *beside = pl.pallas_call(
        functools.partial(project_kernel, len(pieces), len(sources) if inside else 0),
        out_shape=(
            jax.ShapeDtypeStruct(resid.shape, jnp.float32),
            jax.ShapeDtypeStruct(resid.shape, jnp.bfloat16),
            half,
            half,
        ),
        in_specs=[SMALL] + [LOCAL] * (2 * len(pieces) + 2),
        scratch_shapes=[pltpu.VMEM(resid.shape, jnp.float32)],
        name="project", compiler_params=room(20),
    )(jnp.stack(sources).astype(jnp.int32), *pieces, *weights, resid, gain)
    if not inside:
        cuts = [lax.dynamic_slice_in_dim(normed, at * depth, depth, 1) for at in sources]
        normed = jnp.concatenate(cuts, axis=1)
        turned = jnp.concatenate([cuts[k ^ 1] for k in range(len(cuts))], axis=1)
        beside = [turned[: half.shape[0]], turned[half.shape[0] :]]
    return mixed, normed, beside


def pack_kernel(*refs):
    for k, part in enumerate(refs[:-1]):
        refs[-1][k] = part[...]


def pack(parts):
    return pl.pallas_call(
        pack_kernel,
        out_shape=jax.ShapeDtypeStruct((len(parts),) + parts[0].shape, parts[0].dtype),
        compiler_params=room(8),
    )(*parts)


def up_kernel(blocks, steps, *refs):
    rows = refs[:blocks]
    mine = refs[blocks : blocks + steps]
    theirs = refs[blocks + steps : blocks + 2 * steps]
    out, row_buf = refs[blocks + 2 * steps :]
    each, depth, width = mine[0].shape
    at = 0
    for source in rows:
        row_buf[at : at + source.shape[0]] = source[...]
        at += source.shape[0]
    span = each * depth
    for core, weights in enumerate((mine, theirs)):
        here = None
        for k, weight in enumerate(weights):
            part = jnp.dot(
                row_buf[:, k * span : (k + 1) * span],
                weight[...].reshape(span, width),
                preferred_element_type=jnp.float32,
            )
            here = part if here is None else here + part
        out[:, core * width : (core + 1) * width] = jnp.square(jnp.maximum(here, 0.0)).astype(
            jnp.bfloat16
        )


def up_product(rows, mine, theirs):
    steps = len(mine)
    width = mine[0].shape[2]
    total = sum(r.shape[0] for r in rows)
    return pl.pallas_call(
        functools.partial(up_kernel, len(rows), steps),
        out_shape=jax.ShapeDtypeStruct((total, 2 * width), jnp.bfloat16),
        scratch_shapes=[pltpu.VMEM((total, rows[0].shape[1]), jnp.bfloat16)],
        compiler_params=room(26),
    )(*rows, *mine, *theirs)


def split_of(line_first):
    return ((0, 2), (1, 3)) if line_first else ((0, 1), (2, 3))


def down_kernel(orders, early, late, *refs):
    groups = len(orders)
    weights = refs[: 2 * groups]
    outs = refs[2 * groups : 4 * groups]
    wide = refs[4 * groups]
    half = early.shape[1] // 2
    rows = (early.shape[0] + late.shape[0]) // 4
    width = weights[0].shape[2]
    for g, line_first in enumerate(orders):
        for core in range(2):
            for k in range(2):
                wide[core * half : (core + 1) * half, k * width : (k + 1) * width] = weights[
                    2 * g + core
                ][k]
        keep, send = outs[2 * g : 2 * g + 2]
        kept, sent = split_of(line_first)
        first = 0
        for hidden in (early, late):
            part = jnp.dot(hidden[...], wide[...], preferred_element_type=jnp.float32)
            for k in range(hidden.shape[0] // rows):
                value = part[k * rows : (k + 1) * rows]
                block = first + k
                if block in kept:
                    at = kept.index(block) * rows
                    keep[at : at + rows] = value
                    continue
                at = sent.index(block) * rows
                value = value.astype(jnp.bfloat16)
                if line_first:
                    send[at : at + rows, :width] = value[:, width:]
                    send[at : at + rows, width:] = value[:, :width]
                else:
                    send[at : at + rows] = value
            first += hidden.shape[0] // rows


def down_product(early, late, weights, orders):
    half = (early.shape[0] + late.shape[0]) // 2
    width = 2 * weights[0][0].shape[2]
    shapes = [
        jax.ShapeDtypeStruct((half, width), kind)
        for _ in orders
        for kind in (jnp.float32, jnp.bfloat16)
    ]
    flat = [w for pair in weights for w in pair]
    return pl.pallas_call(
        functools.partial(down_kernel, orders),
        out_shape=shapes,
        scratch_shapes=[pltpu.VMEM((early.shape[1], width), jnp.bfloat16)],
        compiler_params=room(18),
    )(early, late, *flat)


def add_kernel(kept, sent, turn, ours, theirs, keep, send):
    rows = keep.shape[0] // len(kept)
    add = lambda k: (
        ours[k * rows : (k + 1) * rows].astype(jnp.float32)
        + theirs[k * rows : (k + 1) * rows].astype(jnp.float32)
    )
    for at, k in enumerate(kept):
        keep[at * rows : (at + 1) * rows] = add(k)
    half = send.shape[1] // 2
    for at, k in enumerate(sent):
        value = add(k).astype(jnp.bfloat16)
        span = slice(at * rows, (at + 1) * rows)
        if turn:
            send[span, :half] = value[:, half:]
            send[span, half:] = value[:, :half]
        else:
            send[span] = value


def add_blocks(ours, theirs, kept, sent, turn):
    rows = ours.shape[0] // (len(kept) + len(sent))
    width = ours.shape[1]
    return pl.pallas_call(
        functools.partial(add_kernel, kept, sent, turn),
        out_shape=(
            jax.ShapeDtypeStruct((rows * len(kept), width), jnp.float32),
            jax.ShapeDtypeStruct((rows * len(sent), width), jnp.bfloat16),
        ),
        compiler_params=room(5),
    )(ours, theirs)


def finish_kernel(count, info, mixed, *refs):
    kept, got, out = refs[:count], refs[count : 2 * count], refs[-1]
    width = kept[0].shape[1] // 2
    for k in range(2 * count):
        at = pl.multiple_of(info[k] * width, LANES)
        cols = slice((k % 2) * width, (k % 2 + 1) * width)
        total = mixed[:, pl.ds(at, width)] + kept[k // 2][:, cols]
        total = total + got[k // 2][:, cols].astype(jnp.float32)
        out[:, pl.ds(at, width)] = total.astype(jnp.bfloat16)


def finish(sources, mixed, kept, got):
    width = kept[0].shape[1] // 2
    if width % LANES == 0:
        return pl.pallas_call(
            functools.partial(finish_kernel, len(kept)),
            out_shape=jax.ShapeDtypeStruct(mixed.shape, jnp.bfloat16),
            in_specs=[SMALL] + [LOCAL] * (1 + 2 * len(kept)),
            name="finish", compiler_params=room(8),
        )(jnp.stack(sources).astype(jnp.int32), mixed, *kept, *got)
    out = jnp.zeros(mixed.shape, jnp.bfloat16)
    for k, source in enumerate(sources):
        cols = slice((k % 2) * width, (k % 2 + 1) * width)
        total = lax.dynamic_slice_in_dim(mixed, source * width, width, 1) + kept[k // 2][:, cols]
        total = total + got[k // 2][:, cols].astype(jnp.float32)
        out = lax.dynamic_update_slice_in_dim(out, total.astype(jnp.bfloat16), source * width, 1)
    return out


def tp_slots():
    outer, a, c = places("tp")
    return [2 * ((d // 2 - a) % outer) + ((d % 2) ^ c) for d in range(2 * outer)]


def tp_exchange(blocks):
    got = [blocks[0]]
    for slot, block in enumerate(blocks[1:], 1):
        step, cross = slot // 2, slot % 2
        got.append(shift(block, "tp", step, cross))
    return got


def tp_weights(value):
    outer = places("tp")[0]
    got = []
    for step in range(outer):
        here = shift(value, "tp", step) if step else value
        got += [here, flip(here, "tp")]
    return got


def row_blocks(value, given):
    outer = places("tp")[0]
    assert outer == 2
    across = shift(value, "tp", 1)
    beside = [neighbour(x) for x in given]
    late = [shift(x, "tp", 1) for x in beside]
    return [value, *beside, across], late


def sum_back(keep, send, line_first):
    across = lambda x: shift(x, "tp", 1)
    along = lambda x: neighbour(x)
    hops = (along, across) if line_first else (across, along)
    keep, send = add_blocks(keep, hops[0](send), (0,), (1,), not line_first)
    return keep, hops[1](send)


def half_shards(shard, dim):
    outer, a, _ = places("sp")
    size = shard.shape[dim] // 2
    kept = lax.dynamic_slice_in_dim(shard, (a % 2) * size, size, dim)
    given = lax.dynamic_slice_in_dim(shard, (1 - a % 2) * size, size, dim)
    steps = [[kept, neighbour(given)]]
    for step in range(1, outer // 2):
        first = shift(steps[-1][0], "sp", 2)
        if step == 1:
            second = skew(given)
        else:
            second = shift(steps[-1][1], "sp", 2)
        steps.append([first, second])
    return steps


def both_cores(packed):
    return packed, flip(packed, "tp")


def up_shards(shard):
    mine, theirs = [], []
    for here in half_shards(shard, 1):
        there = [flip(x, "sp") for x in here]
        packed = pack(here + there)
        mine.append(packed)
        theirs.append(flip(packed, "tp"))
    return mine, theirs


def down_shards(shard):
    got = []
    for here in half_shards(shard, 0):
        packed = pack(here)
        there = [flip(x, "sp") for x in here]
        there = pack(there)
        got.append(both_cores(packed))
        got.append(both_cores(there))
    return got


def ring_sources():
    outer, a, c = places("sp")
    assert outer % 2 == 0
    return [
        2 * (((a - 2 * step) % outer) ^ k) + (c ^ cross)
        for step in range(outer // 2)
        for cross in range(2)
        for k in range(2)
    ]


def shards(
    queries,
    keys,
    values,
    out_gate,
    input_gates,
    forget_gates,
    doc_ids,
    head_gain,
    w_out,
    resid,
    norm_gain,
    w_up,
    w_down,
):
    length = queries.shape[0]
    heads = input_gates.shape[1]
    outer, a, c = places("sp")
    up_mine, up_theirs = up_shards(w_up)
    down_groups = down_shards(w_down)
    out_shards = tp_weights(w_out)

    reach = min(2 * outer - 1, -(-(LONGEST_DOC - 1) // length))
    hops = min(outer - 1, -(-reach // 2))
    doc_pos = doc_ids.astype(jnp.float32)[None]
    slots = tp_slots()
    info = jnp.stack([c, jnp.where(c == 1, a, outer - 1 - a)] + slots).astype(jnp.int32)
    readouts = []
    for h in range(heads):
        cut = lambda x: x.reshape(length, heads, -1)[:, h]
        k, v = cut(keys), cut(values)
        gates = jnp.concatenate(
            [input_gates[:, h], forget_gates[:, h], doc_pos, jnp.zeros((3, length), jnp.float32)]
        )
        give, mine = summaries(info, k, v, gates)
        got = flip(give, "sp")
        pair = pair_state(mine, got)
        ahead = [carry_shift(pair, j) for j in range(1, hops + 1)]
        handed = flip(lead_state(info, ahead), "sp")
        inner = intra(cut(queries), k, v, gates)
        gain = head_gain.reshape(heads, 1, -1)[h]
        readouts.append(
            emit(
                info, cut(queries), inner, cut(out_gate), gain, [got] + ahead, handed, len(slots)
            )
        )
    blocks = readouts[0]
    if heads > 1:
        blocks = [jnp.concatenate(b, axis=1) for b in zip(*readouts)]
    sources = ring_sources()
    mixed, normed, given = project(
        tp_exchange(blocks), out_shards, resid, norm_gain[None], sources, w_up.shape[0]
    )
    early, late = row_blocks(normed, given)
    early = up_product(early, up_mine, up_theirs)
    late = up_product(late, up_mine, up_theirs)

    parts = down_product(early, late, down_groups[:2], (False, True))
    for step in range(2, len(down_groups)):
        parts += down_product(early, late, down_groups[step : step + 1], (step % 2 == 1,))
    kept, got = [], []
    for step in range(len(down_groups)):
        keep, send = parts[2 * step : 2 * step + 2]
        keep, last = sum_back(keep, send, step % 2 == 1)
        kept.append(keep)
        got.append(last)
    return finish(sources, mixed, kept, got)


def solution(mesh):
    in_specs = (
        P("sp", "tp"),
        P("sp", "tp"),
        P("sp", "tp"),
        P("sp", "tp"),
        P(None, "tp", "sp"),
        P(None, "tp", "sp"),
        P("sp"),
        P("tp"),
        P("tp", None),
        P(("sp", "tp"), None),
        P(),
        P("sp", "tp"),
        P("tp", "sp"),
    )
    out_specs = P(("sp", "tp"), None)

    return jax.shard_map(shards, mesh=mesh, in_specs=in_specs, out_specs=out_specs, check_vma=False)
```
